128 devices in a mesh: sp: 32 (over z, y, core), tp: 4 (over x).
Axes of the slice: x: 4, y: 4, z: 4, core: 2. Of those that a mesh axis runs over, the one named last changes fastest.
Arguments:
- activations: bfloat16 [2, 1024, 1024], P(None, 'sp', 'tp'), may hold values from -6 to 6
- norm_gain: float32 [4, 1024], replicated, may hold values from 0.1 to 1.9
- in_weight: bfloat16 [4, 1024, 512], P(None, 'sp', 'tp'), may hold values from -0.1875 to 0.1875
- out_weight: bfloat16 [4, 512, 1024], P(None, 'tp', 'sp'), may hold values from -0.25 to 0.25
- mixing: bfloat16 [4, 4, 128, 128], P(None, 'tp', 'sp'), may hold values from -0.5 to 0.5
- pool_scale: float32 [4, 512], P(None, 'tp'), may hold values from 0.1 to 1.9
Outputs:
- result: bfloat16 [2, 1024, 1024], P(None, 'sp', 'tp')
The draws below stay inside these ranges and needn't reach their ends.
All inputs are finite; a program needn't handle non-finite values.
Results may differ from the reference program's by a relative error of at most 0.03.
Values may be sent and summed in bfloat16 or wider, within the bound.
No kernel may reach another device: no remote copies, remote signals or barrier semaphores. Data moves between devices by JAX's collectives and lax.ppermute only.
A program may use at most 64 MiB of HBM per device.

```python
import jax
import jax.numpy as jnp
from jax import lax

D = 1024
P_SIZE = 512
GROUPS = 4
G = 128
LAYERS = 4
SEQS = 2
SEQ = 1024


def block_scale(own_key, shape, pieces, low, largest):
    level, own = 1.0, jax.random.fold_in(own_key, 6)
    for dim, shards_of in pieces:
        steps = jnp.exp(jax.random.uniform(jax.random.fold_in(own, dim), (shards_of,), jnp.float32, low / len(pieces), largest / len(pieces)))
        level = level * jnp.repeat(steps, shape[dim] // shards_of).reshape([-1 if axis == dim else 1 for axis in range(len(shape))])
    return level


def normal_values(rng, extent, deviation, limit, pieces=(), held_as=jnp.bfloat16):
    drawn = deviation * jax.random.normal(rng, extent, jnp.float32)
    if pieces:
        drawn = drawn * block_scale(rng, extent, pieces, -0.22, 0.18)
    return jnp.clip(drawn, -limit, limit).astype(held_as)


def setup_inputs(seed: int = 0) -> dict:
    arg_keys = jax.random.split(jax.random.key(seed), 7)
    activations = normal_values(arg_keys[0], (SEQS, SEQ, D), 1.0, 6.0, ((1, 32), (2, 4)))
    norm_gain = jnp.clip(1.0 + 0.18 * jax.random.normal(arg_keys[1], (LAYERS, D), jnp.float32), 0.1, 1.9)
    in_weight = normal_values(arg_keys[2], (LAYERS, D, P_SIZE), D ** -0.5, 0.1875, ((1, 32), (2, 4)))
    out_weight = normal_values(arg_keys[3], (LAYERS, P_SIZE, D), P_SIZE ** -0.5, 0.25, ((1, 4), (2, 32)))
    mixing = normal_values(arg_keys[4], (LAYERS, GROUPS, G, G), G ** -0.5, 0.5, ((1, 4), (2, 32)))
    pool_scale = jnp.clip(1.0 + 0.18 * jax.random.normal(arg_keys[5], (LAYERS, P_SIZE), jnp.float32), 0.1, 1.9)
    return dict(activations=activations, norm_gain=norm_gain, in_weight=in_weight, out_weight=out_weight, mixing=mixing, pool_scale=pool_scale)


def pool_layer(activations, norm_gain, in_weight, out_weight, mixing, pool_scale):
    num_seqs, length, model_width = activations.shape
    state_f32 = activations.astype(jnp.float32)
    normed = (state_f32 * lax.rsqrt(lax.optimization_barrier(jnp.mean(state_f32 * state_f32, axis=-1, keepdims=True)) + 1e-06) * norm_gain).astype(jnp.bfloat16)
    flat_rows = normed.reshape(num_seqs * length, model_width)
    pooled_in = jnp.dot(flat_rows, in_weight, preferred_element_type=jnp.float32).astype(jnp.bfloat16)
    pooled_in = pooled_in.reshape(num_seqs, length, -1)
    totals = jnp.pad(jnp.cumsum(pooled_in.astype(jnp.float32), axis=1), ((0, 0), (1, 0), (0, 0)))
    positions = jnp.arange(length, dtype=jnp.int32)
    group_width = mixing.shape[1]
    outputs = []
    for group_slot in range(mixing.shape[0]):
        window = 2 ** (group_slot + 1)
        window_low = jnp.clip(positions - window // 2, 0, length)
        window_high = jnp.clip(positions - window // 2 + window, 0, length)
        columns = slice(group_slot * group_width, (group_slot + 1) * group_width)
        part_sums = totals[:, window_high, columns] - totals[:, window_low, columns]
        window_mean = part_sums / (window_high - window_low).astype(jnp.float32)[None, :, None]
        centred = (window_mean - pooled_in[..., columns].astype(jnp.float32)).astype(jnp.bfloat16)
        mixed_group = jnp.einsum('btc,cd->btd', centred.astype(jnp.float32), mixing[group_slot].astype(jnp.float32))
        outputs.append(mixed_group * pool_scale[columns])
    joined = jnp.concatenate(outputs, axis=-1).astype(jnp.bfloat16).reshape(num_seqs * length, -1)
    next_state = jnp.dot(joined, out_weight, preferred_element_type=jnp.float32).astype(jnp.bfloat16)
    return next_state.reshape(num_seqs, length, model_width)

def reference(activations, norm_gain, in_weight, out_weight, mixing, pool_scale):
    state_now = activations
    for layer_index in range(LAYERS):
        state_now = pool_layer(state_now, norm_gain[layer_index], in_weight[layer_index], out_weight[layer_index], mixing[layer_index], pool_scale[layer_index])
    return state_now
```

```python
import functools

import jax
import jax.numpy as jnp
from jax import lax
from jax.experimental import pallas as pl
from jax.experimental.pallas import tpu as pltpu
from jax.sharding import PartitionSpec as P

NZ, NY, NC, NX = 4, 4, 2, 4
AXES = ("sp", "tp")


def flat(z, y, c, x):
    return (((z % NZ) * NY + y % NY) * NC + c) * NX + x % NX


def pairs(source_of):
    return [
        (flat(*source_of(z, y, c, x)), flat(z, y, c, x))
        for z in range(NZ)
        for y in range(NY)
        for c in range(NC)
        for x in range(NX)
    ]


def from_z(k):
    return pairs(lambda z, y, c, x: (z + k, y, c, x))


def from_x(k):
    return pairs(lambda z, y, c, x: (z, y, c, x + k))


def from_u(k):
    return pairs(lambda z, y, c, x: (z, y + k * c, c, x + k * (1 - c)))


def from_v(k):
    return pairs(lambda z, y, c, x: (z, y + k * (1 - c), c, x + k * c))


def from_core():
    return pairs(lambda z, y, c, x: (z, y, 1 - c, x))


def across_chips():
    count = NZ * NY * NC
    swap = []
    for low in range(1, count - 1, 2):
        for x in range(NX):
            swap += [(low * NX + x, (low + 1) * NX + x), ((low + 1) * NX + x, low * NX + x)]
    return swap


def send(value, perm):
    return lax.ppermute(value, AXES, perm)


def kernel(dims, place, *refs):
    layers, seqs, tok, halo, seq_len = dims
    own, other, acts = refs[0:4], refs[4:8], refs[8:12]
    gain, out = refs[12:14]
    w_in, w_out, mix_raw, state_parts, scales = refs[14:]
    z, y, c, x = (place[k] for k in range(4))
    slab = 64 * layers
    for source, core in ((own, c), (other, 1 - c)):
        first = core == 0
        for k in range(4):
            for j in range(4):
                y_at = lax.rem(y + jnp.where(first, k, j), NY)
                x_at = lax.rem(x + jnp.where(first, j, k), NX)
                for m in range(4):
                    block = lax.rem(z + m, NZ) * (NY * NC) + y_at * NC + core
                    rows = pl.ds(pl.multiple_of(block * 32, 32), 32)
                    for l in range(layers):
                        w_in[l, x_at, rows, :] = source[k][j, m, 64 * l : 64 * l + 32, :]
                        w_out[l, x_at, rows, :] = source[k][j, m, 64 * l + 32 : 64 * l + 64, :]
                    mix_rows = pl.ds(pl.multiple_of(block * 16, 16), 16)
                    mix_raw[x_at, mix_rows, :] = source[k][j, m, slab : slab + 16, :]
    span = tok + 2 * halo
    rows = seqs * span
    for k in range(4):
        x_at = lax.rem(x + k, NX)
        state_parts[x_at] = acts[k][:rows, :]
        parts = acts[k][rows : rows + 16, :128].astype(jnp.float32)
        scales[x_at] = parts[0:layers] + parts[layers : 2 * layers] + parts[2 * layers : 3 * layers]
    i0 = (z * NY + y) * NC + c
    r = lax.broadcasted_iota(jnp.int32, (rows, rows), 0)
    q = lax.broadcasted_iota(jnp.int32, (rows, rows), 1)
    same = (r >= span) == (q >= span)
    start = i0 * tok - halo
    pos_r = start + jnp.where(r >= span, r - span, r)
    pos_q = start + jnp.where(q >= span, q - span, q)
    r1 = lax.broadcasted_iota(jnp.int32, (rows, 1), 0)
    pos_1 = start + jnp.where(r1 >= span, r1 - span, r1)
    bands, inverse = [], []
    for g in range(4):
        half = 2**g
        low = jnp.clip(pos_r - half, 0, seq_len)
        high = jnp.clip(pos_r + half, 0, seq_len)
        bands.append(
            jnp.where(same & (pos_q >= low) & (pos_q < high), 1.0, 0.0).astype(jnp.bfloat16)
        )
        count = jnp.clip(pos_1 + half, 0, seq_len) - jnp.clip(pos_1 - half, 0, seq_len)
        inverse.append(1.0 / jnp.maximum(count, 1).astype(jnp.float32))

    pick_r = lax.broadcasted_iota(jnp.int32, (128, 512), 0)
    pick_q = lax.broadcasted_iota(jnp.int32, (128, 512), 1)
    raw = jnp.concatenate([mix_raw[g] for g in range(4)], axis=1)

    state = jnp.concatenate([state_parts[k] for k in range(4)], axis=1).astype(jnp.float32)
    for l in range(layers):
        pick = jnp.where(pick_q == (pick_r // 4) * 16 + 4 * l + pick_r % 4, 1.0, 0.0)
        mixing = jnp.dot(
            pick.astype(jnp.bfloat16), raw, preferred_element_type=jnp.float32
        ).astype(jnp.bfloat16)
        mean = jnp.mean(state * state, axis=-1, keepdims=True)
        normed = (state * lax.rsqrt(mean + 1e-06) * gain[l : l + 1, :]).astype(jnp.bfloat16)
        mixed = []
        for g in range(4):
            pooled = jnp.dot(normed, w_in[l, g], preferred_element_type=jnp.float32).astype(
                jnp.bfloat16
            )
            sums = jnp.dot(bands[g], pooled, preferred_element_type=jnp.float32)
            centred = (sums * inverse[g] - pooled.astype(jnp.float32)).astype(jnp.bfloat16)
            product = jnp.dot(
                centred,
                mixing[:, 128 * g : 128 * (g + 1)],
                preferred_element_type=jnp.float32,
            )
            mixed.append(
                (product * scales[g, l : l + 1, :]).astype(jnp.bfloat16)
            )
        mixed = jnp.concatenate(mixed, axis=1)
        contract = (((1,), (1,)), ((), ()))
        if l < layers - 1:
            weights = jnp.concatenate([w_out[l, g] for g in range(4)], axis=1)
            state = lax.dot_general(mixed, weights, contract, preferred_element_type=jnp.float32)
            state = state.astype(jnp.bfloat16).astype(jnp.float32)
        else:
            mixed = jnp.concatenate(
                [mixed[s * span + halo : s * span + halo + tok] for s in range(seqs)], axis=0
            )
            width = out.shape[-1]
            columns = pl.ds(pl.multiple_of(x * width, width), width)
            weights = jnp.concatenate([w_out[l, g, columns, :] for g in range(4)], axis=1)
            last = lax.dot_general(mixed, weights, contract, preferred_element_type=jnp.float32)
            out[...] = last.astype(jnp.bfloat16)


def scale_rows(scale, width):
    high = lax.reduce_precision(scale, 8, 7)
    middle = lax.reduce_precision(scale - high, 8, 7)
    terms = jnp.concatenate([high, middle, scale - high - middle]).astype(jnp.bfloat16)
    return jnp.pad(terms, ((0, 16 - terms.shape[0]), (0, width - terms.shape[1])))


def body(activations, norm_gain, in_weight, out_weight, mixing, pool_scale):
    layers = in_weight.shape[0]
    seqs, tok, width = activations.shape
    i, x = lax.axis_index("sp"), lax.axis_index("tp")
    z, y, c = i // (NY * NC), (i // NC) % NY, i % NC
    seq_len = tok * NZ * NY * NC

    pair = jnp.stack([in_weight, jnp.swapaxes(out_weight, 1, 2)], axis=1)
    slab = jnp.concatenate([pair.reshape(64 * layers, 128), mixing.reshape(4 * layers, 128)])

    chip_mate = send(activations, from_core())
    next_chip = send(activations, across_chips())
    left = jnp.where(c == 0, next_chip, chip_mate)
    right = jnp.where(c == 0, chip_mate, next_chip)
    wide = jnp.concatenate([left, activations, right], axis=1)
    wide = wide.reshape(seqs * 3 * tok, width)
    wide = jnp.concatenate([wide, scale_rows(pool_scale, width)])

    by_z = jnp.stack([slab] + [send(slab, from_z(k)) for k in (1, 2, 3)])
    by_u = jnp.stack([by_z] + [send(by_z, from_u(k)) for k in (1, 2, 3)])
    own = [by_u] + [send(by_u, from_v(k)) for k in (1, 2, 3)]
    acts = [wide] + [send(wide, from_x(k)) for k in (1, 2, 3)]
    other = [send(part, from_core()) for part in own]

    place = jnp.stack([z, y, c, x]).astype(jnp.int32)
    vmem = pl.BlockSpec(memory_space=pltpu.VMEM)
    rows = seqs * 3 * tok
    result = pl.pallas_call(
        functools.partial(kernel, (layers, seqs, tok, tok, seq_len)),
        out_shape=jax.ShapeDtypeStruct((seqs * tok, width), jnp.bfloat16),
        in_specs=[pl.BlockSpec(memory_space=pltpu.SMEM)] + [vmem] * 13,
        out_specs=vmem,
        scratch_shapes=[
            pltpu.VMEM((layers, 4, 1024, 128), jnp.bfloat16),
            pltpu.VMEM((layers, 4, 1024, 128), jnp.bfloat16),
            pltpu.VMEM((4, 512, 128), jnp.bfloat16),
            pltpu.VMEM((4, rows, width), jnp.bfloat16),
            pltpu.VMEM((4, layers, 128), jnp.float32),
        ],
        compiler_params=pltpu.CompilerParams(vmem_limit_bytes=48 * 2**20),
        cost_estimate=pl.CostEstimate(
            flops=2 * 10**9, bytes_accessed=18 * 10**6, transcendentals=1000
        ),
    )(place, *own, *other, *acts, norm_gain)
    return result.reshape(seqs, tok, width)


def solution(mesh):
    return jax.shard_map(
        body,
        mesh=mesh,
        in_specs=(
            P(None, "sp", "tp"),
            P(),
            P(None, "sp", "tp"),
            P(None, "tp", "sp"),
            P(None, "tp", "sp", None),
            P(None, "tp"),
        ),
        out_specs=P(None, "sp", "tp"),
        check_vma=False,
    )
```

```python
import functools

import jax
import jax.numpy as jnp
from jax import lax
from jax.experimental import pallas as pl
from jax.experimental.pallas import tpu as pltpu
from jax.sharding import PartitionSpec as P

NZ, NY, NC, NX = 4, 4, 2, 4
AXES = ("sp", "tp")


def flat(z, y, c, x):
    return (((z % NZ) * NY + y % NY) * NC + c) * NX + x % NX


def pairs(source_of):
    return [
        (flat(*source_of(z, y, c, x)), flat(z, y, c, x))
        for z in range(NZ)
        for y in range(NY)
        for c in range(NC)
        for x in range(NX)
    ]


def from_z(k):
    return pairs(lambda z, y, c, x: (z + k, y, c, x))


def from_x(k):
    return pairs(lambda z, y, c, x: (z, y, c, x + k))


def from_u(k):
    return pairs(lambda z, y, c, x: (z, y + k * c, c, x + k * (1 - c)))


def from_v(k):
    return pairs(lambda z, y, c, x: (z, y + k * (1 - c), c, x + k * c))


def from_core():
    return pairs(lambda z, y, c, x: (z, y, 1 - c, x))


def across_chips():
    count = NZ * NY * NC
    swap = []
    for low in range(1, count - 1, 2):
        for x in range(NX):
            swap += [(low * NX + x, (low + 1) * NX + x), ((low + 1) * NX + x, low * NX + x)]
    return swap


def send(value, perm):
    return lax.ppermute(value, AXES, perm)


def blocks(place, source, core, first_row):
    z, y, _, x = place
    column, across, along, corner = source
    first = core == 0
    for k in range(4):
        for j in range(4):
            y_at = lax.rem(y + jnp.where(first, k, j), NY)
            x_at = lax.rem(x + jnp.where(first, j, k), NX)
            for m in range(4):
                index = lax.rem(z + m, NZ) * (NY * NC) + y_at * NC + core
                if k == 0 and j == 0:
                    yield x_at, index, lambda lo, hi: column[m, first_row + lo : first_row + hi, :]
                elif k == 0:
                    yield x_at, index, lambda lo, hi: across[j - 1, m, lo:hi, :]
                elif j == 0:
                    yield (
                        x_at,
                        index,
                        lambda lo, hi: along[k - 1][m, first_row + lo : first_row + hi, :],
                    )
                else:
                    yield x_at, index, lambda lo, hi: corner[k - 1][j - 1, m, lo:hi, :]


def assemble(place, sources, first_row, counts, w_in, w_out, mix_raw=None):
    for source, core in sources:
        for x_at, index, take in blocks(place, source, core, first_row):
            rows = pl.ds(pl.multiple_of(index * 32, 32), 32)
            for l in range(counts):
                w_in[l, x_at, rows, :] = take(64 * l, 64 * l + 32)
                w_out[l, x_at, rows, :] = take(64 * l + 32, 64 * l + 64)
            if mix_raw is not None:
                mix_rows = pl.ds(pl.multiple_of(index * 16, 16), 16)
                mix_raw[x_at, mix_rows, :] = take(64 * counts, 64 * counts + 16)


def windows(start, seqs, span, seq_len):
    rows = seqs * span
    r = lax.broadcasted_iota(jnp.int32, (rows, rows), 0)
    q = lax.broadcasted_iota(jnp.int32, (rows, rows), 1)
    same = (r >= span) == (q >= span)
    pos_r = start + jnp.where(r >= span, r - span, r)
    pos_q = start + jnp.where(q >= span, q - span, q)
    r1 = lax.broadcasted_iota(jnp.int32, (rows, 1), 0)
    pos_1 = start + jnp.where(r1 >= span, r1 - span, r1)
    bands, inverse = [], []
    for g in range(4):
        half = 2**g
        low = jnp.clip(pos_r - half, 0, seq_len)
        high = jnp.clip(pos_r + half, 0, seq_len)
        bands.append(
            jnp.where(same & (pos_q >= low) & (pos_q < high), 1.0, 0.0).astype(jnp.bfloat16)
        )
        count = jnp.clip(pos_1 + half, 0, seq_len) - jnp.clip(pos_1 - half, 0, seq_len)
        inverse.append(1.0 / jnp.maximum(count, 1).astype(jnp.float32))
    return bands, inverse


def mix_layer(state, gain, w_in, scales, mixing, bands, inverse):
    mean = jnp.mean(state * state, axis=-1, keepdims=True)
    normed = (state * lax.rsqrt(mean + 1e-06) * gain).astype(jnp.bfloat16)
    weights = jnp.concatenate([w_in[g] for g in range(4)], axis=1)
    pooled = jnp.dot(normed, weights, preferred_element_type=jnp.float32).astype(jnp.bfloat16)
    mixed = []
    for g in range(4):
        part = pooled[:, 128 * g : 128 * (g + 1)]
        sums = jnp.dot(bands[g], part, preferred_element_type=jnp.float32)
        centred = (sums * inverse[g] - part.astype(jnp.float32)).astype(jnp.bfloat16)
        product = jnp.dot(
            centred, mixing[:, 128 * g : 128 * (g + 1)], preferred_element_type=jnp.float32
        )
        mixed.append((product * scales[g]).astype(jnp.bfloat16))
    return jnp.concatenate(mixed, axis=1)


def project_out(mixed, w_out):
    weights = jnp.concatenate([w_out(g) for g in range(4)], axis=1)
    out = lax.dot_general(
        mixed, weights, (((1,), (1,)), ((), ())), preferred_element_type=jnp.float32
    )
    return out.astype(jnp.bfloat16)


def split(refs):
    return refs[0], refs[1], refs[2:5], refs[5:8]


def first_half(dims, place_ref, *refs):
    layers, seqs, tok, halo, seq_len = dims
    own, other, acts, gain = split(refs[0:8]), split(refs[8:16]), refs[16:20], refs[20]
    state_out, mix_out, scale_out = refs[21:24]
    w_in, w_out, mix_raw, state_parts, scales = refs[24:]
    place = tuple(place_ref[k] for k in range(4))
    z, y, c, x = place
    half = layers // 2
    assemble(place, ((own, c), (other, 1 - c)), 0, half, w_in, w_out, mix_raw)
    span = tok + 2 * halo
    rows = seqs * span
    for k in range(4):
        x_at = lax.rem(x + k, NX)
        state_parts[x_at] = acts[k][:rows, :]
        parts = acts[k][rows : rows + 16, :128].astype(jnp.float32)
        scales[x_at] = parts[0:layers] + parts[layers : 2 * layers] + parts[2 * layers : 3 * layers]
    scale_out[...] = scales[...]
    bands, inverse = windows(((z * NY + y) * NC + c) * tok - halo, seqs, span, seq_len)

    pick_r = lax.broadcasted_iota(jnp.int32, (128, 512), 0)
    pick_q = lax.broadcasted_iota(jnp.int32, (128, 512), 1)
    base = ((pick_r >> 2) << 4) + (pick_r & 3)
    raw = jnp.concatenate([mix_raw[g] for g in range(4)], axis=1)
    mixings = []
    for l in range(layers):
        pick = jnp.where(pick_q == base + 4 * l, 1.0, 0.0).astype(jnp.bfloat16)
        mixings.append(
            jnp.dot(pick, raw, preferred_element_type=jnp.float32).astype(jnp.bfloat16)
        )
    for l in range(half, layers):
        mix_out[l - half] = mixings[l]

    state = jnp.concatenate([state_parts[k] for k in range(4)], axis=1)
    for l in range(half):
        row = [scales[g, l : l + 1, :] for g in range(4)]
        mixed = mix_layer(
            state.astype(jnp.float32),
            gain[l : l + 1, :],
            [w_in[l, g] for g in range(4)],
            row,
            mixings[l],
            bands,
            inverse,
        )
        state = project_out(mixed, lambda g: w_out[l, g])
    state_out[...] = state


def second_half(dims, place_ref, *refs):
    layers, seqs, tok, halo, seq_len = dims
    own, other = split(refs[0:8]), split(refs[8:16])
    state_in, mix_in, scales, gain, out, w_in, w_out = refs[16:]
    place = tuple(place_ref[k] for k in range(4))
    z, y, c, x = place
    half = layers // 2
    assemble(place, ((own, c), (other, 1 - c)), 64 * half + 16, half, w_in, w_out)
    span = tok + 2 * halo
    bands, inverse = windows(((z * NY + y) * NC + c) * tok - halo, seqs, span, seq_len)
    state = state_in[...]
    for l in range(half):
        at = half + l
        row = [scales[g, at : at + 1, :] for g in range(4)]
        mixed = mix_layer(
            state.astype(jnp.float32),
            gain[at : at + 1, :],
            [w_in[l, g] for g in range(4)],
            row,
            mix_in[l],
            bands,
            inverse,
        )
        if l < half - 1:
            state = project_out(mixed, lambda g: w_out[l, g])
        else:
            mixed = jnp.concatenate(
                [mixed[s * span + halo : s * span + halo + tok] for s in range(seqs)], axis=0
            )
            width = out.shape[-1]
            columns = pl.ds(pl.multiple_of(x * width, width), width)
            out[...] = project_out(mixed, lambda g: w_out[l, g, columns, :])


def scale_rows(scale, width):
    high = lax.reduce_precision(scale, 8, 7)
    middle = lax.reduce_precision(scale - high, 8, 7)
    terms = jnp.concatenate([high, middle, scale - high - middle]).astype(jnp.bfloat16)
    return jnp.pad(terms, ((0, 16 - terms.shape[0]), (0, width - terms.shape[1])))


def body(activations, norm_gain, in_weight, out_weight, mixing, pool_scale):
    layers = in_weight.shape[0]
    half = layers // 2
    seqs, tok, width = activations.shape
    i, x = lax.axis_index("sp"), lax.axis_index("tp")
    z, y, c = i // (NY * NC), (i // NC) % NY, i % NC
    seq_len = tok * NZ * NY * NC
    cut = 64 * half + 16

    pair = jnp.stack([in_weight, jnp.swapaxes(out_weight, 1, 2)], axis=1)
    pair = pair.reshape(64 * layers, 128)
    slab = jnp.concatenate(
        [pair[: 64 * half], mixing.reshape(4 * layers, 128), pair[64 * half :]]
    )
    column = jnp.stack([slab] + [send(slab, from_z(k)) for k in (1, 2, 3)])
    chip_mate = send(activations, from_core())
    next_chip = send(activations, across_chips())
    left = jnp.where(c == 0, next_chip, chip_mate)
    right = jnp.where(c == 0, chip_mate, next_chip)
    wide = jnp.concatenate([left, activations, right], axis=1)
    wide = wide.reshape(seqs * 3 * tok, width)
    wide = jnp.concatenate([wide, scale_rows(pool_scale, width)])

    across = jnp.stack([send(column, from_u(k)) for k in (1, 2, 3)])
    along = [send(column, from_v(k)) for k in (1, 2, 3)]
    early, late = across[:, :, :cut, :], across[:, :, cut:, :]
    corner_early = [send(early, from_v(k)) for k in (1, 2, 3)]
    acts = [wide] + [send(wide, from_x(k)) for k in (1, 2, 3)]
    corner_late = [send(late, from_v(k)) for k in (1, 2, 3)]
    column_2 = send(column, from_core())
    early_2 = send(early, from_core())
    along_2 = [send(part, from_core()) for part in along]
    late_2 = send(late, from_core())
    corner_early_2 = [send(part, from_core()) for part in corner_early]
    corner_late_2 = [send(part, from_core()) for part in corner_late]

    place = jnp.stack([z, y, c, x]).astype(jnp.int32)
    vmem = pl.BlockSpec(memory_space=pltpu.VMEM)
    smem = pl.BlockSpec(memory_space=pltpu.SMEM)
    rows = seqs * 3 * tok
    dims = (layers, seqs, tok, tok, seq_len)
    weights = pltpu.VMEM((half, 4, 1024, 128), jnp.bfloat16)
    params = pltpu.CompilerParams(vmem_limit_bytes=20 * 2**20)
    cost = pl.CostEstimate(flops=10**9, bytes_accessed=9 * 10**6, transcendentals=1000)
    state, mix_late, scales = pl.pallas_call(
        functools.partial(first_half, dims),
        out_shape=(
            jax.ShapeDtypeStruct((rows, NX * width), jnp.bfloat16),
            jax.ShapeDtypeStruct((layers - half, 128, 512), jnp.bfloat16),
            jax.ShapeDtypeStruct((4, layers, 128), jnp.float32),
        ),
        in_specs=[smem] + [vmem] * 21,
        out_specs=(vmem, vmem, vmem),
        scratch_shapes=[
            weights,
            weights,
            pltpu.VMEM((4, 512, 128), jnp.bfloat16),
            pltpu.VMEM((4, rows, width), jnp.bfloat16),
            pltpu.VMEM((4, layers, 128), jnp.float32),
        ],
        compiler_params=params,
        cost_estimate=cost,
        name="first_half",
    )(
        place,
        column,
        early,
        *along,
        *corner_early,
        column_2,
        early_2,
        *along_2,
        *corner_early_2,
        *acts,
        norm_gain,
    )
    result = pl.pallas_call(
        functools.partial(second_half, dims),
        out_shape=jax.ShapeDtypeStruct((seqs * tok, width), jnp.bfloat16),
        in_specs=[smem] + [vmem] * 20,
        out_specs=vmem,
        scratch_shapes=[weights, weights],
        compiler_params=params,
        cost_estimate=cost,
        name="second_half",
    )(
        place,
        column,
        late,
        *along,
        *corner_late,
        column_2,
        late_2,
        *along_2,
        *corner_late_2,
        state,
        mix_late,
        scales,
        norm_gain,
    )
    return result.reshape(seqs, tok, width)


def solution(mesh):
    return jax.shard_map(
        body,
        mesh=mesh,
        in_specs=(
            P(None, "sp", "tp"),
            P(),
            P(None, "sp", "tp"),
            P(None, "tp", "sp"),
            P(None, "tp", "sp", None),
            P(None, "tp"),
        ),
        out_specs=P(None, "sp", "tp"),
        check_vma=False,
    )
```

```python
import functools

import jax
import jax.numpy as jnp
from jax import lax
from jax.experimental import pallas as pl
from jax.experimental.pallas import tpu as pltpu
from jax.sharding import PartitionSpec as P

NZ, NY, NC, NX = 4, 4, 2, 4
AXES = ("sp", "tp")


def flat(z, y, c, x):
    return (((z % NZ) * NY + y % NY) * NC + c) * NX + x % NX


def pairs(source_of):
    return [
        (flat(*source_of(z, y, c, x)), flat(z, y, c, x))
        for z in range(NZ)
        for y in range(NY)
        for c in range(NC)
        for x in range(NX)
    ]


def from_z(k):
    return pairs(lambda z, y, c, x: (z + k, y, c, x))


def from_u(k):
    return pairs(lambda z, y, c, x: (z, y + k * c, c, x + k * (1 - c)))


def from_v(k):
    return pairs(lambda z, y, c, x: (z, y + k * (1 - c), c, x + k * c))


def from_core():
    return pairs(lambda z, y, c, x: (z, y, 1 - c, x))


def across_chips():
    count = NZ * NY * NC
    swap = []
    for low in range(1, count - 1, 2):
        for x in range(NX):
            swap += [(low * NX + x, (low + 1) * NX + x), ((low + 1) * NX + x, low * NX + x)]
    return swap


def send(value, perm):
    return lax.ppermute(value, AXES, perm)


def copy_blocks(place, sources, steps, copy):
    z, y, _, x = place
    for parts, core in sources:
        first = core == 0
        for k in range(4):
            for m in range(4):
                for j in range(4):
                    step = dict(zip(steps, (k, m, j)))
                    y_at = lax.rem(y + jnp.where(first, step["v"], step["u"]), NY)
                    x_at = lax.rem(x + jnp.where(first, step["u"], step["v"]), NX)
                    index = lax.rem(z + step["z"], NZ) * (NY * NC) + y_at * NC + core
                    copy(x_at, index, parts[k].at[m, j])


def put_layers(layers, w_in, w_out, mix_raw=None):
    def copy(x_at, index, part):
        rows = pl.ds(pl.multiple_of(index * 32, 32), 32)
        for at, l in enumerate(layers):
            w_in[l, x_at, rows, :] = part[64 * at : 64 * at + 32, :]
            w_out[l, x_at, rows, :] = part[64 * at + 32 : 64 * at + 64, :]
        if mix_raw is not None:
            end = 64 * len(layers)
            mix_rows = pl.ds(pl.multiple_of(index * 16, 16), 16)
            mix_raw[x_at, mix_rows, :] = part[end : end + 16, :]

    return copy


def windows(start, seqs, span, seq_len):
    rows = seqs * span
    r = lax.broadcasted_iota(jnp.int32, (rows, rows), 0)
    q = lax.broadcasted_iota(jnp.int32, (rows, rows), 1)
    same = (r >= span) == (q >= span)
    pos_r = start + jnp.where(r >= span, r - span, r)
    pos_q = start + jnp.where(q >= span, q - span, q)
    r1 = lax.broadcasted_iota(jnp.int32, (rows, 1), 0)
    pos_1 = start + jnp.where(r1 >= span, r1 - span, r1)
    bands, inverse = [], []
    for g in range(4):
        half = 2**g
        low = jnp.clip(pos_r - half, 0, seq_len)
        high = jnp.clip(pos_r + half, 0, seq_len)
        bands.append(
            jnp.where(same & (pos_q >= low) & (pos_q < high), 1.0, 0.0).astype(jnp.bfloat16)
        )
        count = jnp.clip(pos_1 + half, 0, seq_len) - jnp.clip(pos_1 - half, 0, seq_len)
        inverse.append(1.0 / jnp.maximum(count, 1).astype(jnp.float32))
    return bands, inverse


def mix_layer(state, gain, w_in, scales, mixing, bands, inverse):
    mean = jnp.mean(state * state, axis=-1, keepdims=True)
    normed = (state * lax.rsqrt(mean + 1e-06) * gain).astype(jnp.bfloat16)
    weights = jnp.concatenate([w_in[g] for g in range(4)], axis=1)
    pooled = jnp.dot(normed, weights, preferred_element_type=jnp.float32).astype(jnp.bfloat16)
    mixed = []
    for g in range(4):
        part = pooled[:, 128 * g : 128 * (g + 1)]
        sums = jnp.dot(bands[g], part, preferred_element_type=jnp.float32)
        centred = (sums * inverse[g] - part.astype(jnp.float32)).astype(jnp.bfloat16)
        product = jnp.dot(
            centred, mixing[:, 128 * g : 128 * (g + 1)], preferred_element_type=jnp.float32
        )
        mixed.append((product * scales[g]).astype(jnp.bfloat16))
    return jnp.concatenate(mixed, axis=1)


def project_out(mixed, w_out):
    weights = jnp.concatenate([w_out(g) for g in range(4)], axis=1)
    out = lax.dot_general(
        mixed, weights, (((1,), (1,)), ((), ())), preferred_element_type=jnp.float32
    )
    return out.astype(jnp.bfloat16)


def first_half(dims, place_ref, *refs):
    layers, seqs, tok, halo, seq_len = dims
    own, other, acts, beside, gain = refs[0:4], refs[4:8], refs[8], refs[9], refs[10]
    state_out, mix_out, scale_out = refs[11:14]
    w_in, w_out, mix_raw, state_parts, scales = refs[14:]
    place = tuple(place_ref[k] for k in range(4))
    z, y, c, x = place
    half = layers // 2
    put = put_layers(range(half), w_in, w_out, mix_raw)
    copy_blocks(place, ((own, c), (other, 1 - c)), "vzu", put)
    span = tok + 2 * halo
    for k in range(4):
        x_at = lax.rem(x + k, NX)
        for h in range(2):
            lanes = slice(128 * h, 128 * (h + 1))
            for s in range(seqs):
                for core in range(NC):
                    low = ((h * NC + core) * seqs + s) * tok
                    at = pl.ds(pl.multiple_of(s * span + (1 + core - c) * tok, tok), tok)
                    state_parts[x_at, at, lanes] = acts[k, low : low + tok, :]
                low = (h * seqs + s) * tok
                at = pl.ds(pl.multiple_of(s * span + 2 * c * tok, tok), tok)
                state_parts[x_at, at, lanes] = beside[k, low : low + tok, :]
        parts = acts[k, 4 * seqs * tok : 4 * seqs * tok + 16, :].astype(jnp.float32)
        scales[x_at] = parts[0:layers] + parts[layers : 2 * layers] + parts[2 * layers : 3 * layers]
    scale_out[...] = scales[...]
    bands, inverse = windows(((z * NY + y) * NC + c) * tok - halo, seqs, span, seq_len)

    pick_r = lax.broadcasted_iota(jnp.int32, (128, 512), 0)
    pick_q = lax.broadcasted_iota(jnp.int32, (128, 512), 1)
    base = ((pick_r >> 2) << 4) + (pick_r & 3)
    raw = jnp.concatenate([mix_raw[g] for g in range(4)], axis=1)
    mixings = []
    for l in range(layers):
        pick = jnp.where(pick_q == base + 4 * l, 1.0, 0.0).astype(jnp.bfloat16)
        mixings.append(
            jnp.dot(pick, raw, preferred_element_type=jnp.float32).astype(jnp.bfloat16)
        )
    for l in range(half, layers):
        mix_out[l - half] = mixings[l]

    state = jnp.concatenate([state_parts[k] for k in range(4)], axis=1)
    for l in range(half):
        row = [scales[g, l : l + 1, :] for g in range(4)]
        mixed = mix_layer(
            state.astype(jnp.float32),
            gain[l : l + 1, :],
            [w_in[l, g] for g in range(4)],
            row,
            mixings[l],
            bands,
            inverse,
        )
        state = project_out(mixed, lambda g: w_out[l, g])
    state_out[...] = state


def second_half(dims, place_ref, *refs):
    layers, seqs, tok, halo, seq_len = dims
    state_in, mix_in, scales, gain, out, w_in, w_out = refs[16:]
    place = tuple(place_ref[k] for k in range(4))
    z, y, c, x = place
    half = layers // 2
    third = ((refs[0:4], c), (refs[4:8], 1 - c))
    fourth = ((refs[8:12], c), (refs[12:16], 1 - c))
    copy_blocks(place, third, "vzu", put_layers((0,), w_in, w_out))
    copy_blocks(place, fourth, "zvu", put_layers((1,), w_in, w_out))
    span = tok + 2 * halo
    bands, inverse = windows(((z * NY + y) * NC + c) * tok - halo, seqs, span, seq_len)
    state = state_in[...]
    for l in range(half):
        at = half + l
        row = [scales[g, at : at + 1, :] for g in range(4)]
        mixed = mix_layer(
            state.astype(jnp.float32),
            gain[at : at + 1, :],
            [w_in[l, g] for g in range(4)],
            row,
            mix_in[l],
            bands,
            inverse,
        )
        if l < half - 1:
            state = project_out(mixed, lambda g: w_out[l, g])
        else:
            mixed = jnp.concatenate(
                [mixed[s * span + halo : s * span + halo + tok] for s in range(seqs)], axis=0
            )
            width = out.shape[-1]
            columns = pl.ds(pl.multiple_of(x * width, width), width)
            out[...] = project_out(mixed, lambda g: w_out[l, g, columns, :])


def scale_rows(scale):
    high = lax.reduce_precision(scale, 8, 7)
    middle = lax.reduce_precision(scale - high, 8, 7)
    terms = jnp.concatenate([high, middle, scale - high - middle]).astype(jnp.bfloat16)
    return jnp.pad(terms, ((0, 16 - terms.shape[0]), (0, 0)))


def body(activations, norm_gain, in_weight, out_weight, mixing, pool_scale):
    layers = in_weight.shape[0]
    half = layers // 2
    seqs, tok, width = activations.shape
    i, x = lax.axis_index("sp"), lax.axis_index("tp")
    z, y, c = i // (NY * NC), (i // NC) % NY, i % NC
    seq_len = tok * NZ * NY * NC
    cuts = (64 * half + 16, 64 * half + 80, 64 * half + 144)

    chip_mate = send(activations, from_core())
    both = jnp.where(
        c == 0, jnp.stack([activations, chip_mate]), jnp.stack([chip_mate, activations])
    ).reshape(NC * seqs * tok, width)
    pair = jnp.stack([in_weight, jnp.swapaxes(out_weight, 1, 2)], axis=1)
    pair = pair.reshape(64 * layers, 128)
    message = jnp.concatenate(
        [
            pair[: 64 * half],
            mixing.reshape(4 * layers, 128),
            pair[64 * half :],
            both[:, :128],
            both[:, 128:],
            scale_rows(pool_scale),
        ]
    )
    got = [message] + [send(message, from_u(k)) for k in (1, 2, 3)]
    ab = jnp.stack([part[: cuts[1]] for part in got])
    q = jnp.stack([part[cuts[1] : cuts[2]] for part in got])
    tokens = jnp.stack([part[cuts[2] :] for part in got])
    tokens_2 = send(tokens, from_core())
    tokens = jnp.where(c == 0, tokens, tokens_2)

    ab = [ab] + [send(ab, from_z(k)) for k in (1, 2, 3)]
    q = jnp.stack([q] + [send(q, from_v(k)) for k in (1, 2, 3)])
    mine = tokens[:, : 2 * NC * seqs * tok, :].reshape(4, 2, NC, seqs * tok, 128)
    mine = jnp.where(c == 0, mine[:, :, 0], mine[:, :, 1]).reshape(4, 2 * seqs * tok, 128)
    beside = send(mine, across_chips())
    a = jnp.stack([part[:, : cuts[0]] for part in ab])
    b = jnp.stack([part[:, cuts[0] :] for part in ab])
    a = [a] + [send(a, from_v(k)) for k in (1, 2, 3)]
    q = [q] + [send(q, from_z(k)) for k in (1, 2, 3)]
    b = [b] + [send(b, from_v(k)) for k in (1, 2, 3)]
    a_2 = [send(part, from_core()) for part in a]
    b_2 = [send(b[0], from_core())]
    q_2 = [send(q[0], from_core())]
    b_2 += [send(part, from_core()) for part in b[1:]]
    q_2 += [send(part, from_core()) for part in q[1:]]

    place = jnp.stack([z, y, c, x]).astype(jnp.int32)
    vmem = pl.BlockSpec(memory_space=pltpu.VMEM)
    smem = pl.BlockSpec(memory_space=pltpu.SMEM)
    rows = seqs * 3 * tok
    dims = (layers, seqs, tok, tok, seq_len)
    weights = pltpu.VMEM((half, 4, 1024, 128), jnp.bfloat16)
    params = pltpu.CompilerParams(vmem_limit_bytes=14 * 2**20)
    cost = pl.CostEstimate(flops=10**9, bytes_accessed=9 * 10**6, transcendentals=1000)
    state, mix_late, scales = pl.pallas_call(
        functools.partial(first_half, dims),
        out_shape=(
            jax.ShapeDtypeStruct((rows, NX * width), jnp.bfloat16),
            jax.ShapeDtypeStruct((layers - half, 128, 512), jnp.bfloat16),
            jax.ShapeDtypeStruct((4, layers, 128), jnp.float32),
        ),
        in_specs=[smem] + [vmem] * 11,
        out_specs=(vmem, vmem, vmem),
        scratch_shapes=[
            weights,
            weights,
            pltpu.VMEM((4, 512, 128), jnp.bfloat16),
            pltpu.VMEM((4, rows, width), jnp.bfloat16),
            pltpu.VMEM((4, layers, 128), jnp.float32),
        ],
        compiler_params=params,
        cost_estimate=cost,
        name="first_half",
    )(
        place,
        *a,
        *a_2,
        tokens,
        beside,
        norm_gain,
    )
    result = pl.pallas_call(
        functools.partial(second_half, dims),
        out_shape=jax.ShapeDtypeStruct((seqs * tok, width), jnp.bfloat16),
        in_specs=[smem] + [vmem] * 20,
        out_specs=vmem,
        scratch_shapes=[weights, weights],
        compiler_params=params,
        cost_estimate=cost,
        name="second_half",
    )(
        place,
        *b,
        *b_2,
        *q,
        *q_2,
        state,
        mix_late,
        scales,
        norm_gain,
    )
    return result.reshape(seqs, tok, width)


def solution(mesh):
    return jax.shard_map(
        body,
        mesh=mesh,
        in_specs=(
            P(None, "sp", "tp"),
            P(),
            P(None, "sp", "tp"),
            P(None, "tp", "sp"),
            P(None, "tp", "sp", None),
            P(None, "tp"),
        ),
        out_specs=P(None, "sp", "tp"),
        check_vma=False,
    )
```

```python
import functools

import jax
import jax.numpy as jnp
from jax import lax
from jax.experimental import pallas as pl
from jax.experimental.pallas import tpu as pltpu
from jax.sharding import PartitionSpec as P

NZ, NY, NC, NX = 4, 4, 2, 4
AXES = ("sp", "tp")


def flat(z, y, c, x):
    return (((z % NZ) * NY + y % NY) * NC + c) * NX + x % NX


def pairs(source_of):
    return [
        (flat(*source_of(z, y, c, x)), flat(z, y, c, x))
        for z in range(NZ)
        for y in range(NY)
        for c in range(NC)
        for x in range(NX)
    ]


def from_z(k):
    return pairs(lambda z, y, c, x: (z + k, y, c, x))


def from_u(k):
    return pairs(lambda z, y, c, x: (z, y + k * c, c, x + k * (1 - c)))


def from_v(k):
    return pairs(lambda z, y, c, x: (z, y + k * (1 - c), c, x + k * c))


def from_core():
    return pairs(lambda z, y, c, x: (z, y, 1 - c, x))


def across_chips():
    count = NZ * NY * NC
    swap = []
    for low in range(1, count - 1, 2):
        for x in range(NX):
            swap += [(low * NX + x, (low + 1) * NX + x), ((low + 1) * NX + x, low * NX + x)]
    return swap


def send(value, perm):
    return lax.ppermute(value, AXES, perm)


def copy_blocks(place, sources, steps, copy):
    z, y, _, x = place
    for parts, core in sources:
        first = core == 0
        for k in range(4):
            for m in range(4):
                for j in range(4):
                    step = dict(zip(steps, (k, m, j)))
                    y_at = lax.rem(y + jnp.where(first, step["v"], step["u"]), NY)
                    x_at = lax.rem(x + jnp.where(first, step["u"], step["v"]), NX)
                    index = lax.rem(z + step["z"], NZ) * (NY * NC) + y_at * NC + core
                    copy(x_at, index, parts[k].at[m, j])


def put_layers(layers, w_in, w_out, mix_raw=None):
    def copy(x_at, index, part):
        rows = pl.ds(pl.multiple_of(index * 32, 32), 32)
        for at, l in enumerate(layers):
            w_in[l, x_at, rows, :] = part[64 * at : 64 * at + 32, :]
            w_out[l, x_at, rows, :] = part[64 * at + 32 : 64 * at + 64, :]
        if mix_raw is not None:
            end = 64 * len(layers)
            mix_rows = pl.ds(pl.multiple_of(index * 16, 16), 16)
            mix_raw[x_at, mix_rows, :] = part[end : end + 16, :]

    return copy


def windows(start, seqs, span, seq_len):
    rows = seqs * span
    r = lax.broadcasted_iota(jnp.int32, (rows, rows), 0)
    q = lax.broadcasted_iota(jnp.int32, (rows, rows), 1)
    same = (r >= span) == (q >= span)
    pos_r = start + jnp.where(r >= span, r - span, r)
    pos_q = start + jnp.where(q >= span, q - span, q)
    r1 = lax.broadcasted_iota(jnp.int32, (rows, 1), 0)
    pos_1 = start + jnp.where(r1 >= span, r1 - span, r1)
    bands, inverse = [], []
    for g in range(4):
        half = 2**g
        low = jnp.clip(pos_r - half, 0, seq_len)
        high = jnp.clip(pos_r + half, 0, seq_len)
        bands.append(
            jnp.where(same & (pos_q >= low) & (pos_q < high), 1.0, 0.0).astype(jnp.bfloat16)
        )
        count = jnp.clip(pos_1 + half, 0, seq_len) - jnp.clip(pos_1 - half, 0, seq_len)
        inverse.append(1.0 / jnp.maximum(count, 1).astype(jnp.float32))
    return bands, inverse


def mix_layer(state, gain, w_in, scales, mixing, bands, inverse):
    mean = jnp.mean(state * state, axis=-1, keepdims=True)
    normed = (state * lax.rsqrt(mean + 1e-06) * gain).astype(jnp.bfloat16)
    weights = jnp.concatenate([w_in[g] for g in range(4)], axis=1)
    pooled = jnp.dot(normed, weights, preferred_element_type=jnp.float32).astype(jnp.bfloat16)
    mixed = []
    for g in range(4):
        part = pooled[:, 128 * g : 128 * (g + 1)]
        sums = jnp.dot(bands[g], part, preferred_element_type=jnp.float32)
        centred = (sums * inverse[g] - part.astype(jnp.float32)).astype(jnp.bfloat16)
        product = jnp.dot(
            centred, mixing[:, 128 * g : 128 * (g + 1)], preferred_element_type=jnp.float32
        )
        mixed.append((product * scales[g]).astype(jnp.bfloat16))
    return jnp.concatenate(mixed, axis=1)


def project_out(mixed, w_out):
    weights = jnp.concatenate([w_out(g) for g in range(4)], axis=1)
    out = lax.dot_general(
        mixed, weights, (((1,), (1,)), ((), ())), preferred_element_type=jnp.float32
    )
    return out.astype(jnp.bfloat16)


def first_half(dims, place_ref, *refs):
    layers, seqs, tok, halo, seq_len = dims
    own, other, acts, beside, gain = refs[0:4], refs[4:8], refs[8], refs[9], refs[10]
    state_out, mix_out, scale_out = refs[11:14]
    w_in, w_out, mix_raw, state_parts, scales = refs[14:]
    place = tuple(place_ref[k] for k in range(4))
    z, y, c, x = place
    half = layers // 2
    put = put_layers(range(half), w_in, w_out, mix_raw)
    copy_blocks(place, ((own, c), (other, 1 - c)), "vzu", put)
    span = tok + 2 * halo
    for k in range(4):
        x_at = lax.rem(x + k, NX)
        for h in range(2):
            lanes = slice(128 * h, 128 * (h + 1))
            for s in range(seqs):
                for core in range(NC):
                    low = 16 + ((core * 2 + h) * seqs + s) * tok
                    at = pl.ds(pl.multiple_of(s * span + (1 + core - c) * tok, tok), tok)
                    state_parts[x_at, at, lanes] = acts[k, low : low + tok, :]
                low = (h * seqs + s) * tok
                at = pl.ds(pl.multiple_of(s * span + 2 * c * tok, tok), tok)
                state_parts[x_at, at, lanes] = beside[k, low : low + tok, :]
        parts = acts[k, 0:16, :].astype(jnp.float32)
        scales[x_at] = parts[0:layers] + parts[layers : 2 * layers] + parts[2 * layers : 3 * layers]
    scale_out[...] = scales[...]
    bands, inverse = windows(((z * NY + y) * NC + c) * tok - halo, seqs, span, seq_len)

    pick_r = lax.broadcasted_iota(jnp.int32, (128, 512), 0)
    pick_q = lax.broadcasted_iota(jnp.int32, (128, 512), 1)
    base = ((pick_r >> 2) << 4) + (pick_r & 3)
    raw = jnp.concatenate([mix_raw[g] for g in range(4)], axis=1)
    mixings = []
    for l in range(layers):
        pick = jnp.where(pick_q == base + 4 * l, 1.0, 0.0).astype(jnp.bfloat16)
        mixings.append(
            jnp.dot(pick, raw, preferred_element_type=jnp.float32).astype(jnp.bfloat16)
        )
    for l in range(half, layers):
        mix_out[l - half] = mixings[l]

    state = jnp.concatenate([state_parts[k] for k in range(4)], axis=1)
    for l in range(half):
        row = [scales[g, l : l + 1, :] for g in range(4)]
        mixed = mix_layer(
            state.astype(jnp.float32),
            gain[l : l + 1, :],
            [w_in[l, g] for g in range(4)],
            row,
            mixings[l],
            bands,
            inverse,
        )
        state = project_out(mixed, lambda g: w_out[l, g])
    state_out[...] = state


def second_half(dims, place_ref, *refs):
    layers, seqs, tok, halo, seq_len = dims
    state_in, mix_in, scales, gain, out, w_in, w_out = refs[16:]
    place = tuple(place_ref[k] for k in range(4))
    z, y, c, x = place
    half = layers // 2
    third = ((refs[0:4], c), (refs[4:8], 1 - c))
    fourth = ((refs[8:12], c), (refs[12:16], 1 - c))
    copy_blocks(place, third, "vzu", put_layers((0,), w_in, w_out))
    copy_blocks(place, fourth, "zvu", put_layers((1,), w_in, w_out))
    span = tok + 2 * halo
    bands, inverse = windows(((z * NY + y) * NC + c) * tok - halo, seqs, span, seq_len)
    state = state_in[...]
    for l in range(half):
        at = half + l
        row = [scales[g, at : at + 1, :] for g in range(4)]
        mixed = mix_layer(
            state.astype(jnp.float32),
            gain[at : at + 1, :],
            [w_in[l, g] for g in range(4)],
            row,
            mix_in[l],
            bands,
            inverse,
        )
        if l < half - 1:
            state = project_out(mixed, lambda g: w_out[l, g])
        else:
            mixed = jnp.concatenate(
                [mixed[s * span + halo : s * span + halo + tok] for s in range(seqs)], axis=0
            )
            width = out.shape[-1]
            columns = pl.ds(pl.multiple_of(x * width, width), width)
            out[...] = project_out(mixed, lambda g: w_out[l, g, columns, :])


def pack(layers, place_ref, in_ref, out_ref, mix_ref, scale_ref, act_ref, gain_ref, message, gain):
    half = layers // 2
    row = 0
    for l in range(layers):
        message[row : row + 32, :] = in_ref[l]
        message[row + 32 : row + 64, :] = out_ref[l]
        row += 64
        if l == half - 1:
            mix = jnp.concatenate([mix_ref[k].astype(jnp.float32) for k in range(layers)])
            message[row : row + 16, :] = mix.astype(jnp.bfloat16)
            row += 16
    scale = scale_ref[...]
    high = scale.astype(jnp.bfloat16).astype(jnp.float32)
    middle = (scale - high).astype(jnp.bfloat16).astype(jnp.float32)
    terms = jnp.concatenate([high, middle, scale - high - middle, jnp.zeros_like(scale)])
    message[row : row + 16, :] = terms.astype(jnp.bfloat16)
    row += 16
    seqs, tok, _ = act_ref.shape
    own = row + place_ref[2] * (seqs * tok * 2)
    for h in range(2):
        for s in range(seqs):
            at = pl.ds(pl.multiple_of(own + (h * seqs + s) * tok, 16), tok)
            message[at, :] = act_ref[s, :, 128 * h : 128 * (h + 1)]
    gain[...] = gain_ref[...]


def body(activations, norm_gain, in_weight, out_weight, mixing, pool_scale):
    layers = in_weight.shape[0]
    half = layers // 2
    seqs, tok, width = activations.shape
    i, x = lax.axis_index("sp"), lax.axis_index("tp")
    z, y, c = i // (NY * NC), (i // NC) % NY, i % NC
    seq_len = tok * NZ * NY * NC
    cuts = (64 * half + 16, 64 * half + 80, 64 * half + 144)

    chip_mate = send(activations, from_core())
    place = jnp.stack([z, y, c, x]).astype(jnp.int32)
    vmem = pl.BlockSpec(memory_space=pltpu.VMEM)
    smem = pl.BlockSpec(memory_space=pltpu.SMEM)
    message, gain = pl.pallas_call(
        functools.partial(pack, layers),
        out_shape=(
            jax.ShapeDtypeStruct((cuts[2] + 16 + 4 * seqs * tok, 128), jnp.bfloat16),
            jax.ShapeDtypeStruct(norm_gain.shape, jnp.float32),
        ),
        in_specs=[smem] + [vmem] * 6,
        out_specs=(vmem, vmem),
        compiler_params=pltpu.CompilerParams(vmem_limit_bytes=2**21),
        cost_estimate=pl.CostEstimate(flops=10**6, bytes_accessed=3 * 10**5, transcendentals=0),
        name="pack",
    )(
        place,
        in_weight,
        jnp.swapaxes(out_weight, 1, 2),
        mixing.reshape(layers, 4, 128),
        pool_scale,
        activations,
        norm_gain,
    )
    mate_rows = jnp.concatenate(
        [chip_mate.reshape(seqs * tok, width)[:, 128 * h : 128 * (h + 1)] for h in range(2)]
    )
    mate_at = cuts[2] + 16 + (1 - c) * (2 * seqs * tok)
    message = lax.dynamic_update_slice(message, mate_rows, (mate_at, 0))
    got = [message] + [send(message, from_u(k)) for k in (1, 2, 3)]
    ab = jnp.stack([part[: cuts[1]] for part in got])
    q = jnp.stack([part[cuts[1] : cuts[2]] for part in got])
    tokens = jnp.stack([part[cuts[2] :] for part in got])
    tokens_2 = send(tokens, from_core())
    tokens = jnp.where(c == 0, tokens, tokens_2)

    ab = [ab] + [send(ab, from_z(k)) for k in (1, 2, 3)]
    q = [q] + [send(q, from_v(k)) for k in (1, 2, 3)]
    count = 2 * seqs * tok
    mine = jnp.where(c == 0, tokens[:, 16 : 16 + count], tokens[:, 16 + count :])
    beside = send(mine, across_chips())
    a = jnp.stack([part[:, : cuts[0]] for part in ab])
    b = jnp.stack([part[:, cuts[0] :] for part in ab])
    a = [a] + [send(a, from_v(k)) for k in (1, 2, 3)]
    q = jnp.stack(q)
    q = [q] + [send(q, from_z(k)) for k in (1, 2, 3)]
    b = [b] + [send(b, from_v(k)) for k in (1, 2, 3)]
    a_2 = [send(part, from_core()) for part in a]
    b_2 = [send(b[0], from_core())]
    q_2 = [send(q[0], from_core())]
    b_2 += [send(part, from_core()) for part in b[1:]]
    q_2 += [send(part, from_core()) for part in q[1:]]

    rows = seqs * 3 * tok
    dims = (layers, seqs, tok, tok, seq_len)
    weights = pltpu.VMEM((half, 4, 1024, 128), jnp.bfloat16)
    params = pltpu.CompilerParams(vmem_limit_bytes=14 * 2**20)
    cost = pl.CostEstimate(flops=10**9, bytes_accessed=9 * 10**6, transcendentals=1000)
    state, mix_late, scales = pl.pallas_call(
        functools.partial(first_half, dims),
        out_shape=(
            jax.ShapeDtypeStruct((rows, NX * width), jnp.bfloat16),
            jax.ShapeDtypeStruct((layers - half, 128, 512), jnp.bfloat16),
            jax.ShapeDtypeStruct((4, layers, 128), jnp.float32),
        ),
        in_specs=[smem] + [vmem] * 11,
        out_specs=(vmem, vmem, vmem),
        scratch_shapes=[
            weights,
            weights,
            pltpu.VMEM((4, 512, 128), jnp.bfloat16),
            pltpu.VMEM((4, rows, width), jnp.bfloat16),
            pltpu.VMEM((4, layers, 128), jnp.float32),
        ],
        compiler_params=params,
        cost_estimate=cost,
        name="first_half",
    )(
        place,
        *a,
        *a_2,
        tokens,
        beside,
        gain,
    )
    result = pl.pallas_call(
        functools.partial(second_half, dims),
        out_shape=jax.ShapeDtypeStruct((seqs * tok, width), jnp.bfloat16),
        in_specs=[smem] + [vmem] * 20,
        out_specs=vmem,
        scratch_shapes=[weights, weights],
        compiler_params=params,
        cost_estimate=cost,
        name="second_half",
    )(
        place,
        *b,
        *b_2,
        *q,
        *q_2,
        state,
        mix_late,
        scales,
        gain,
    )
    return result.reshape(seqs, tok, width)


def solution(mesh):
    return jax.shard_map(
        body,
        mesh=mesh,
        in_specs=(
            P(None, "sp", "tp"),
            P(),
            P(None, "sp", "tp"),
            P(None, "tp", "sp"),
            P(None, "tp", "sp", None),
            P(None, "tp"),
        ),
        out_specs=P(None, "sp", "tp"),
        check_vma=False,
    )
```

```python
import functools

import jax
import jax.numpy as jnp
from jax import lax
from jax.experimental import pallas as pl
from jax.experimental.pallas import tpu as pltpu
from jax.sharding import PartitionSpec as P

NZ, NY, NC, NX = 4, 4, 2, 4
AXES = ("sp", "tp")


def flat(z, y, c, x):
    return (((z % NZ) * NY + y % NY) * NC + c) * NX + x % NX


def pairs(source_of):
    return [
        (flat(*source_of(z, y, c, x)), flat(z, y, c, x))
        for z in range(NZ)
        for y in range(NY)
        for c in range(NC)
        for x in range(NX)
    ]


FIRST = ("xzy", "zyx")
LAST = ("xyz", "yxz")


def along(order, step, k):
    def source(z, y, c, x):
        at = dict(z=z, y=y, x=x)
        at[order[c][step]] += k
        return at["z"], at["y"], c, at["x"]

    return pairs(source)


def gather(value, order, step):
    return [send(value, along(order, step, k)) for k in (1, 2, 3)]


def from_core():
    return pairs(lambda z, y, c, x: (z, y, 1 - c, x))


def across_chips():
    count = NZ * NY * NC
    swap = []
    for low in range(1, count - 1, 2):
        for x in range(NX):
            swap += [(low * NX + x, (low + 1) * NX + x), ((low + 1) * NX + x, low * NX + x)]
    return swap


def send(value, perm):
    return lax.ppermute(value, AXES, perm)


def copy_blocks(place, sources, order, copy):
    z, y, _, x = place
    for parts, core in sources:
        first = core == 0
        for k in range(4):
            for m in range(4):
                for j in range(4):
                    north, south = (dict(zip(axes, (j, m, k))) for axes in order)
                    y_at = lax.rem(y + jnp.where(first, north["y"], south["y"]), NY)
                    x_at = lax.rem(x + jnp.where(first, north["x"], south["x"]), NX)
                    z_at = lax.rem(z + jnp.where(first, north["z"], south["z"]), NZ)
                    copy(x_at, z_at * (NY * NC) + y_at * NC + core, parts[k].at[m, j])


def put_layers(layers, w_in, w_out, mix_raw=None):
    def copy(x_at, index, part):
        rows = pl.ds(pl.multiple_of(index * 32, 32), 32)
        for at, l in enumerate(layers):
            w_in[l, x_at, rows, :] = part[64 * at : 64 * at + 32, :]
            w_out[l, x_at, rows, :] = part[64 * at + 32 : 64 * at + 64, :]
        if mix_raw is not None:
            end = 64 * len(layers)
            mix_rows = pl.ds(pl.multiple_of(index * 16, 16), 16)
            mix_raw[x_at, mix_rows, :] = part[end : end + 16, :]

    return copy


def tables(layers, seqs, tok, halo, seq_len, place_ref, bands, inverse, picks):
    z, y, c = (place_ref[k] for k in range(3))
    start = ((z * NY + y) * NC + c) * tok - halo
    span = tok + 2 * halo
    rows = seqs * span
    r = lax.broadcasted_iota(jnp.int32, (rows, rows), 0)
    q = lax.broadcasted_iota(jnp.int32, (rows, rows), 1)
    same = (r >= span) == (q >= span)
    pos_r = start + jnp.where(r >= span, r - span, r)
    pos_q = start + jnp.where(q >= span, q - span, q)
    r1 = lax.broadcasted_iota(jnp.int32, (rows, 128), 0)
    pos_1 = start + jnp.where(r1 >= span, r1 - span, r1)
    for g in range(4):
        half = 2**g
        low = jnp.clip(pos_r - half, 0, seq_len)
        high = jnp.clip(pos_r + half, 0, seq_len)
        inside = same & (pos_q >= low) & (pos_q < high)
        bands[g] = jnp.where(inside, 1.0, 0.0).astype(jnp.bfloat16)
        count = jnp.clip(pos_1 + half, 0, seq_len) - jnp.clip(pos_1 - half, 0, seq_len)
        inverse[g] = 1.0 / jnp.maximum(count, 1).astype(jnp.float32)
    pick_r = lax.broadcasted_iota(jnp.int32, (128, 512), 0)
    pick_q = lax.broadcasted_iota(jnp.int32, (128, 512), 1)
    base = ((pick_r >> 2) << 4) + (pick_r & 3)
    for l in range(layers):
        picks[l] = jnp.where(pick_q == base + 4 * l, 1.0, 0.0).astype(jnp.bfloat16)


def mix_layer(state, gain, w_in, scales, mixing, bands, inverse):
    mean = jnp.mean(state * state, axis=-1, keepdims=True)
    normed = (state * lax.rsqrt(mean + 1e-06) * gain).astype(jnp.bfloat16)
    weights = jnp.concatenate([w_in[g] for g in range(4)], axis=1)
    pooled = jnp.dot(normed, weights, preferred_element_type=jnp.float32).astype(jnp.bfloat16)
    mixed = []
    for g in range(4):
        part = pooled[:, 128 * g : 128 * (g + 1)]
        sums = jnp.dot(bands[g], part, preferred_element_type=jnp.float32)
        centred = (sums * inverse[g] - part.astype(jnp.float32)).astype(jnp.bfloat16)
        product = jnp.dot(
            centred, mixing[:, 128 * g : 128 * (g + 1)], preferred_element_type=jnp.float32
        )
        mixed.append((product * scales[g]).astype(jnp.bfloat16))
    return jnp.concatenate(mixed, axis=1)


def project_out(mixed, w_out):
    weights = jnp.concatenate([w_out(g) for g in range(4)], axis=1)
    out = lax.dot_general(
        mixed, weights, (((1,), (1,)), ((), ())), preferred_element_type=jnp.float32
    )
    return out.astype(jnp.bfloat16)


def first_half(dims, place_ref, *refs):
    layers, seqs, tok, halo, _ = dims
    own, other, acts, beside, gain = refs[0:4], refs[4:8], refs[8], refs[9], refs[10]
    bands, inverse, picks = refs[11:14]
    state_out, mix_out, scale_out = refs[14:17]
    w_in, w_out, mix_raw, state_parts, scales = refs[17:]
    place = tuple(place_ref[k] for k in range(4))
    _, _, c, x = place
    half = layers // 2
    put = put_layers(range(half), w_in, w_out, mix_raw)
    copy_blocks(place, ((own, c), (other, 1 - c)), FIRST, put)
    span = tok + 2 * halo
    for k in range(4):
        x_at = lax.rem(x + k, NX)
        for h in range(2):
            lanes = slice(128 * h, 128 * (h + 1))
            for s in range(seqs):
                for core in range(NC):
                    low = 16 + ((core * 2 + h) * seqs + s) * tok
                    at = pl.ds(pl.multiple_of(s * span + (1 + core - c) * tok, tok), tok)
                    state_parts[x_at, at, lanes] = acts[k, low : low + tok, :]
                low = (h * seqs + s) * tok
                at = pl.ds(pl.multiple_of(s * span + 2 * c * tok, tok), tok)
                state_parts[x_at, at, lanes] = beside[k, low : low + tok, :]
        parts = acts[k, 0:16, :].astype(jnp.float32)
        scales[x_at] = parts[0:layers] + parts[layers : 2 * layers] + parts[2 * layers : 3 * layers]
    scale_out[...] = scales[...]
    raw = jnp.concatenate([mix_raw[g] for g in range(4)], axis=1)
    mixings = []
    for l in range(layers):
        product = jnp.dot(picks[l], raw, preferred_element_type=jnp.float32)
        mixings.append(product.astype(jnp.bfloat16))
    for l in range(half, layers):
        mix_out[l - half] = mixings[l]

    state = jnp.concatenate([state_parts[k] for k in range(4)], axis=1)
    for l in range(half):
        row = [scales[g, l : l + 1, :] for g in range(4)]
        mixed = mix_layer(
            state.astype(jnp.float32),
            gain[l : l + 1, :],
            [w_in[l, g] for g in range(4)],
            row,
            mixings[l],
            bands,
            inverse,
        )
        state = project_out(mixed, lambda g: w_out[l, g])
    state_out[...] = state


def second_half(dims, place_ref, *refs):
    layers, seqs, tok, halo, _ = dims
    state_in, mix_in, scales, gain, bands, inverse, out, w_in, w_out = refs[16:]
    place = tuple(place_ref[k] for k in range(4))
    _, _, c, x = place
    half = layers // 2
    third = ((refs[0:4], c), (refs[4:8], 1 - c))
    fourth = ((refs[8:12], c), (refs[12:16], 1 - c))
    copy_blocks(place, third, FIRST, put_layers((0,), w_in, w_out))
    copy_blocks(place, fourth, LAST, put_layers((1,), w_in, w_out))
    span = tok + 2 * halo
    state = state_in[...]
    for l in range(half):
        at = half + l
        row = [scales[g, at : at + 1, :] for g in range(4)]
        mixed = mix_layer(
            state.astype(jnp.float32),
            gain[at : at + 1, :],
            [w_in[l, g] for g in range(4)],
            row,
            mix_in[l],
            bands,
            inverse,
        )
        if l < half - 1:
            state = project_out(mixed, lambda g: w_out[l, g])
        else:
            mixed = jnp.concatenate(
                [mixed[s * span + halo : s * span + halo + tok] for s in range(seqs)], axis=0
            )
            width = out.shape[-1]
            columns = pl.ds(pl.multiple_of(x * width, width), width)
            out[...] = project_out(mixed, lambda g: w_out[l, g, columns, :])


def pack(
    layers, place_ref, in_ref, out_ref, mix_ref, scale_ref, act_ref, gain_ref, first, last, gain
):
    half = layers // 2
    row = 0
    for l in range(layers - 1):
        first[row : row + 32, :] = in_ref[l]
        first[row + 32 : row + 64, :] = out_ref[l]
        row += 64
        if l == half - 1:
            mix = jnp.concatenate([mix_ref[k].astype(jnp.float32) for k in range(layers)])
            first[row : row + 16, :] = mix.astype(jnp.bfloat16)
            row += 16
    last[0:32, :] = in_ref[layers - 1]
    last[32:64, :] = out_ref[layers - 1]
    scale = scale_ref[...]
    high = scale.astype(jnp.bfloat16).astype(jnp.float32)
    middle = (scale - high).astype(jnp.bfloat16).astype(jnp.float32)
    terms = jnp.concatenate([high, middle, scale - high - middle, jnp.zeros_like(scale)])
    last[64:80, :] = terms.astype(jnp.bfloat16)
    seqs, tok, _ = act_ref.shape
    own = 80 + place_ref[2] * (seqs * tok * 2)
    for h in range(2):
        for s in range(seqs):
            at = pl.ds(pl.multiple_of(own + (h * seqs + s) * tok, 16), tok)
            last[at, :] = act_ref[s, :, 128 * h : 128 * (h + 1)]
    gain[...] = gain_ref[...]


def body(activations, norm_gain, in_weight, out_weight, mixing, pool_scale):
    layers = in_weight.shape[0]
    half = layers // 2
    seqs, tok, width = activations.shape
    i, x = lax.axis_index("sp"), lax.axis_index("tp")
    z, y, c = i // (NY * NC), (i // NC) % NY, i % NC
    seq_len = tok * NZ * NY * NC
    cut = 64 * half + 16
    chip_mate = send(activations, from_core())
    place = jnp.stack([z, y, c, x]).astype(jnp.int32)
    vmem = pl.BlockSpec(memory_space=pltpu.VMEM)
    smem = pl.BlockSpec(memory_space=pltpu.SMEM)
    first, last, gain = pl.pallas_call(
        functools.partial(pack, layers),
        out_shape=(
            jax.ShapeDtypeStruct((cut + 64, 128), jnp.bfloat16),
            jax.ShapeDtypeStruct((80 + 4 * seqs * tok, 128), jnp.bfloat16),
            jax.ShapeDtypeStruct(norm_gain.shape, jnp.float32),
        ),
        in_specs=[smem] + [vmem] * 6,
        out_specs=(vmem, vmem, vmem),
        compiler_params=pltpu.CompilerParams(vmem_limit_bytes=2**21),
        cost_estimate=pl.CostEstimate(flops=10**6, bytes_accessed=3 * 10**5, transcendentals=0),
        name="pack",
    )(
        place,
        in_weight,
        jnp.swapaxes(out_weight, 1, 2),
        mixing.reshape(layers, 4, 128),
        pool_scale,
        activations,
        norm_gain,
    )
    mate_rows = jnp.concatenate(
        [chip_mate.reshape(seqs * tok, width)[:, 128 * h : 128 * (h + 1)] for h in range(2)]
    )
    count = 2 * seqs * tok
    last = lax.dynamic_update_slice(last, mate_rows, (80 + (1 - c) * count, 0))

    got = [first] + gather(first, FIRST, 0)
    got_last = [last] + gather(last, LAST, 0)
    ab = jnp.stack(got)
    ab = [ab] + gather(ab, FIRST, 1)
    q = jnp.stack([part[:64] for part in got_last])
    tokens = jnp.stack([part[64:] for part in got_last])
    tokens_2 = send(tokens, from_core())
    q = [q] + gather(q, LAST, 1)

    a = jnp.stack([part[:, :cut] for part in ab])
    a = [a] + gather(a, FIRST, 2)
    b = jnp.stack([part[:, cut:] for part in ab])
    tokens = jnp.where(c == 0, tokens, tokens_2)
    mine = jnp.where(c == 0, tokens[:, 16 : 16 + count], tokens[:, 16 + count :])
    beside = send(mine, across_chips())
    q = jnp.stack(q)
    q = [q] + gather(q, LAST, 2)
    b = [b] + gather(b, FIRST, 2)
    a_2 = [send(a[0], from_core())]
    b_2 = [send(b[0], from_core())]
    q_2 = [send(q[0], from_core())]
    a_2 += [send(a[1], from_core())]
    a_2 += [send(part, from_core()) for part in a[2:]]
    b_2 += [send(part, from_core()) for part in b[1:]]
    q_2 += [send(part, from_core()) for part in q[1:]]

    rows = seqs * 3 * tok
    dims = (layers, seqs, tok, tok, seq_len)
    bands, inverse, picks = pl.pallas_call(
        functools.partial(tables, *dims),
        out_shape=(
            jax.ShapeDtypeStruct((4, rows, rows), jnp.bfloat16),
            jax.ShapeDtypeStruct((4, rows, 128), jnp.float32),
            jax.ShapeDtypeStruct((layers, 128, 512), jnp.bfloat16),
        ),
        in_specs=[smem],
        out_specs=(vmem, vmem, vmem),
        compiler_params=pltpu.CompilerParams(vmem_limit_bytes=2**22),
        cost_estimate=pl.CostEstimate(flops=10**7, bytes_accessed=10**6, transcendentals=0),
        name="tables",
    )(place)
    weights = pltpu.VMEM((half, 4, 1024, 128), jnp.bfloat16)
    params = pltpu.CompilerParams(vmem_limit_bytes=14 * 2**20)
    cost = pl.CostEstimate(flops=10**9, bytes_accessed=9 * 10**6, transcendentals=1000)
    state, mix_late, scales = pl.pallas_call(
        functools.partial(first_half, dims),
        out_shape=(
            jax.ShapeDtypeStruct((rows, NX * width), jnp.bfloat16),
            jax.ShapeDtypeStruct((layers - half, 128, 512), jnp.bfloat16),
            jax.ShapeDtypeStruct((4, layers, 128), jnp.float32),
        ),
        in_specs=[smem] + [vmem] * 14,
        out_specs=(vmem, vmem, vmem),
        scratch_shapes=[
            weights,
            weights,
            pltpu.VMEM((4, 512, 128), jnp.bfloat16),
            pltpu.VMEM((4, rows, width), jnp.bfloat16),
            pltpu.VMEM((4, layers, 128), jnp.float32),
        ],
        compiler_params=params,
        cost_estimate=cost,
        name="first_half",
    )(
        place,
        *a,
        *a_2,
        tokens,
        beside,
        gain,
        bands,
        inverse,
        picks,
    )
    result = pl.pallas_call(
        functools.partial(second_half, dims),
        out_shape=jax.ShapeDtypeStruct((seqs * tok, width), jnp.bfloat16),
        in_specs=[smem] + [vmem] * 22,
        out_specs=vmem,
        scratch_shapes=[weights, weights],
        compiler_params=params,
        cost_estimate=cost,
        name="second_half",
    )(
        place,
        *b,
        *b_2,
        *q,
        *q_2,
        state,
        mix_late,
        scales,
        gain,
        bands,
        inverse,
    )
    return result.reshape(seqs, tok, width)


def solution(mesh):
    return jax.shard_map(
        body,
        mesh=mesh,
        in_specs=(
            P(None, "sp", "tp"),
            P(),
            P(None, "sp", "tp"),
            P(None, "tp", "sp"),
            P(None, "tp", "sp", None),
            P(None, "tp"),
        ),
        out_specs=P(None, "sp", "tp"),
        check_vma=False,
    )
```

```python
import functools

import jax
import jax.numpy as jnp
from jax import lax
from jax.experimental import pallas as pl
from jax.experimental.pallas import tpu as pltpu
from jax.sharding import PartitionSpec as P

NZ, NY, NC, NX = 4, 4, 2, 4
AXES = ("sp", "tp")


def flat(z, y, c, x):
    return (((z % NZ) * NY + y % NY) * NC + c) * NX + x % NX


def pairs(source_of):
    return [
        (flat(*source_of(z, y, c, x)), flat(z, y, c, x))
        for z in range(NZ)
        for y in range(NY)
        for c in range(NC)
        for x in range(NX)
    ]


FIRST = ("xzy", "zyx")
LAST = ("xyz", "yxz")


def along(order, step, k):
    def source(z, y, c, x):
        at = dict(z=z, y=y, x=x)
        at[order[c][step]] += k
        return at["z"], at["y"], c, at["x"]

    return pairs(source)


def gather(value, order, step):
    return [send(value, along(order, step, k)) for k in (1, 2, 3)]


def from_core():
    return pairs(lambda z, y, c, x: (z, y, 1 - c, x))


def across_chips():
    count = NZ * NY * NC
    swap = []
    for low in range(1, count - 1, 2):
        for x in range(NX):
            swap += [(low * NX + x, (low + 1) * NX + x), ((low + 1) * NX + x, low * NX + x)]
    return swap


def send(value, perm):
    return lax.ppermute(value, AXES, perm)


def copy_blocks(place, sources, order, copy):
    z, y, _, x = place
    for parts, core in sources:
        first = core == 0
        for k in range(4):
            for m in range(4):
                for j in range(4):
                    north, south = (dict(zip(axes, (j, m, k))) for axes in order)
                    y_at = lax.rem(y + jnp.where(first, north["y"], south["y"]), NY)
                    x_at = lax.rem(x + jnp.where(first, north["x"], south["x"]), NX)
                    z_at = lax.rem(z + jnp.where(first, north["z"], south["z"]), NZ)
                    copy(x_at, z_at * (NY * NC) + y_at * NC + core, parts[k].at[m, j])


def put_layers(layers, w_in, w_out, mix_raw=None):
    def copy(x_at, index, part):
        rows = pl.ds(pl.multiple_of(index * 32, 32), 32)
        for at, l in enumerate(layers):
            w_in[l, x_at, rows, :] = part[64 * at : 64 * at + 32, :]
            w_out[l, x_at, rows, :] = part[64 * at + 32 : 64 * at + 64, :]
        if mix_raw is not None:
            end = 64 * len(layers)
            mix_rows = pl.ds(pl.multiple_of(index * 16, 16), 16)
            mix_raw[x_at, mix_rows, :] = part[end : end + 16, :]

    return copy


def tables(layers, seqs, tok, halo, seq_len, place_ref, *refs):
    z, y, c = (place_ref[k] for k in range(3))
    first = ((z * NY + y) * NC + c) * tok
    for beside, bands, inverse in ((halo, *refs[0:2]), (halo // 2, *refs[2:4])):
        start = first - beside
        span = tok + 2 * beside
        rows = seqs * span
        r = lax.broadcasted_iota(jnp.int32, (rows, rows), 0)
        q = lax.broadcasted_iota(jnp.int32, (rows, rows), 1)
        same = (r >= span) == (q >= span)
        pos_r = start + jnp.where(r >= span, r - span, r)
        pos_q = start + jnp.where(q >= span, q - span, q)
        r1 = lax.broadcasted_iota(jnp.int32, (rows, 128), 0)
        pos_1 = start + jnp.where(r1 >= span, r1 - span, r1)
        for g in range(4):
            half = 2**g
            low = jnp.clip(pos_r - half, 0, seq_len)
            high = jnp.clip(pos_r + half, 0, seq_len)
            inside = same & (pos_q >= low) & (pos_q < high)
            bands[g] = jnp.where(inside, 1.0, 0.0).astype(jnp.bfloat16)
            count = jnp.clip(pos_1 + half, 0, seq_len) - jnp.clip(pos_1 - half, 0, seq_len)
            inverse[g] = 1.0 / jnp.maximum(count, 1).astype(jnp.float32)
    picks = refs[4]
    pick_r = lax.broadcasted_iota(jnp.int32, (128, 512), 0)
    pick_q = lax.broadcasted_iota(jnp.int32, (128, 512), 1)
    base = ((pick_r >> 2) << 4) + (pick_r & 3)
    for l in range(layers):
        picks[l] = jnp.where(pick_q == base + 4 * l, 1.0, 0.0).astype(jnp.bfloat16)


def mix_layer(state, gain, w_in, scales, mixing, bands, inverse):
    mean = jnp.mean(state * state, axis=-1, keepdims=True)
    normed = (state * lax.rsqrt(mean + 1e-06) * gain).astype(jnp.bfloat16)
    weights = jnp.concatenate([w_in[g] for g in range(4)], axis=1)
    pooled = jnp.dot(normed, weights, preferred_element_type=jnp.float32).astype(jnp.bfloat16)
    mixed = []
    for g in range(4):
        part = pooled[:, 128 * g : 128 * (g + 1)]
        sums = jnp.dot(bands[g], part, preferred_element_type=jnp.float32)
        centred = (sums * inverse[g] - part.astype(jnp.float32)).astype(jnp.bfloat16)
        product = jnp.dot(
            centred, mixing[:, 128 * g : 128 * (g + 1)], preferred_element_type=jnp.float32
        )
        mixed.append((product * scales[g]).astype(jnp.bfloat16))
    return jnp.concatenate(mixed, axis=1)


def project_out(mixed, w_out):
    weights = jnp.concatenate([w_out(g) for g in range(4)], axis=1)
    out = lax.dot_general(
        mixed, weights, (((1,), (1,)), ((), ())), preferred_element_type=jnp.float32
    )
    return out.astype(jnp.bfloat16)


def inner(rows, seqs, cut):
    span = rows.shape[0] // seqs
    return jnp.concatenate([rows[s * span + cut : (s + 1) * span - cut] for s in range(seqs)])


def all_layers(dims, place_ref, *refs):
    layers, seqs, tok, halo, _ = dims
    acts, beside, gain = refs[16:19]
    wide, narrow, picks, out = refs[19:21], refs[21:23], refs[23], refs[24]
    w_in, w_out, mix_raw, state_parts, scales = refs[25:]
    place = tuple(place_ref[k] for k in range(4))
    _, _, c, x = place
    span = tok + 2 * halo
    for k in range(4):
        x_at = lax.rem(x + k, NX)
        for h in range(2):
            lanes = slice(128 * h, 128 * (h + 1))
            for s in range(seqs):
                for core in range(NC):
                    low = 16 + ((core * 2 + h) * seqs + s) * tok
                    at = pl.ds(pl.multiple_of(s * span + (1 + core - c) * tok, tok), tok)
                    state_parts[x_at, at, lanes] = acts[k, low : low + tok, :]
                low = (h * seqs + s) * tok
                at = pl.ds(pl.multiple_of(s * span + 2 * c * tok, tok), tok)
                state_parts[x_at, at, lanes] = beside[k, low : low + tok, :]
        parts = acts[k, 0:16, :].astype(jnp.float32)
        scales[x_at] = parts[0:layers] + parts[layers : 2 * layers] + parts[2 * layers : 3 * layers]
    put = put_layers(range(layers - 1), w_in, w_out, mix_raw)
    copy_blocks(place, ((refs[0:4], c), (refs[4:8], 1 - c)), FIRST, put)
    put = put_layers((layers - 1,), w_in, w_out)
    copy_blocks(place, ((refs[8:12], c), (refs[12:16], 1 - c)), LAST, put)

    raw = jnp.concatenate([mix_raw[g] for g in range(4)], axis=1)
    state = jnp.concatenate([state_parts[k] for k in range(4)], axis=1)
    for l in range(layers):
        mixing = jnp.dot(picks[l], raw, preferred_element_type=jnp.float32).astype(jnp.bfloat16)
        bands, inverse = wide if l < layers // 2 else narrow
        mixed = mix_layer(
            state.astype(jnp.float32),
            gain[l : l + 1, :],
            [w_in[l, g] for g in range(4)],
            [scales[g, l : l + 1, :] for g in range(4)],
            mixing,
            bands,
            inverse,
        )
        if l == layers // 2 - 1:
            mixed = inner(mixed, seqs, halo // 2)
        if l < layers - 1:
            state = project_out(mixed, lambda g: w_out[l, g])
        else:
            width = out.shape[-1]
            columns = pl.ds(pl.multiple_of(x * width, width), width)
            mixed = inner(mixed, seqs, halo // 2)
            out[...] = project_out(mixed, lambda g: w_out[l, g, columns, :])


def pack(
    layers, place_ref, in_ref, out_ref, mix_ref, scale_ref, act_ref, gain_ref, first, last, gain
):
    for l in range(layers - 1):
        first[64 * l : 64 * l + 32, :] = in_ref[l]
        first[64 * l + 32 : 64 * l + 64, :] = out_ref[l]
    mix = jnp.concatenate([mix_ref[k].astype(jnp.float32) for k in range(layers)])
    first[64 * layers - 64 : 64 * layers - 48, :] = mix.astype(jnp.bfloat16)
    last[0:32, :] = in_ref[layers - 1]
    last[32:64, :] = out_ref[layers - 1]
    scale = scale_ref[...]
    high = scale.astype(jnp.bfloat16).astype(jnp.float32)
    middle = (scale - high).astype(jnp.bfloat16).astype(jnp.float32)
    terms = jnp.concatenate([high, middle, scale - high - middle, jnp.zeros_like(scale)])
    last[64:80, :] = terms.astype(jnp.bfloat16)
    seqs, tok, _ = act_ref.shape
    own = 80 + place_ref[2] * (seqs * tok * 2)
    for h in range(2):
        for s in range(seqs):
            at = pl.ds(pl.multiple_of(own + (h * seqs + s) * tok, 16), tok)
            last[at, :] = act_ref[s, :, 128 * h : 128 * (h + 1)]
    gain[...] = gain_ref[...]


def body(activations, norm_gain, in_weight, out_weight, mixing, pool_scale):
    layers = in_weight.shape[0]
    seqs, tok, width = activations.shape
    i, x = lax.axis_index("sp"), lax.axis_index("tp")
    z, y, c = i // (NY * NC), (i // NC) % NY, i % NC
    seq_len = tok * NZ * NY * NC
    chip_mate = send(activations, from_core())
    place = jnp.stack([z, y, c, x]).astype(jnp.int32)
    vmem = pl.BlockSpec(memory_space=pltpu.VMEM)
    smem = pl.BlockSpec(memory_space=pltpu.SMEM)
    first, last, gain = pl.pallas_call(
        functools.partial(pack, layers),
        out_shape=(
            jax.ShapeDtypeStruct((64 * layers - 48, 128), jnp.bfloat16),
            jax.ShapeDtypeStruct((80 + 4 * seqs * tok, 128), jnp.bfloat16),
            jax.ShapeDtypeStruct(norm_gain.shape, jnp.float32),
        ),
        in_specs=[smem] + [vmem] * 6,
        out_specs=(vmem, vmem, vmem),
        compiler_params=pltpu.CompilerParams(vmem_limit_bytes=2**21),
        cost_estimate=pl.CostEstimate(flops=10**6, bytes_accessed=3 * 10**5, transcendentals=0),
        name="pack",
    )(
        place,
        in_weight,
        jnp.swapaxes(out_weight, 1, 2),
        mixing.reshape(layers, 4, 128),
        pool_scale,
        activations,
        norm_gain,
    )
    mate_rows = jnp.concatenate(
        [chip_mate.reshape(seqs * tok, width)[:, 128 * h : 128 * (h + 1)] for h in range(2)]
    )
    count = 2 * seqs * tok
    last = lax.dynamic_update_slice(last, mate_rows, (80 + (1 - c) * count, 0))

    got = [first] + gather(first, FIRST, 0)
    got_last = [last] + gather(last, LAST, 0)
    p = jnp.stack(got)
    p = [p] + gather(p, FIRST, 1)
    q = jnp.stack([part[:64] for part in got_last])
    tokens = jnp.stack([part[64:] for part in got_last])
    tokens_2 = send(tokens, from_core())
    q = [q] + gather(q, LAST, 1)

    p = jnp.stack(p)
    p = [p] + gather(p, FIRST, 2)
    tokens = jnp.where(c == 0, tokens, tokens_2)
    mine = jnp.where(c == 0, tokens[:, 16 : 16 + count], tokens[:, 16 + count :])
    beside = send(mine, across_chips())
    q = jnp.stack(q)
    q = [q] + gather(q, LAST, 2)
    p_2 = [send(p[0], from_core())]
    q_2 = [send(q[0], from_core())]
    p_2 += [send(part, from_core()) for part in p[1:]]
    q_2 += [send(part, from_core()) for part in q[1:]]

    rows = seqs * 3 * tok
    dims = (layers, seqs, tok, tok, seq_len)
    inner_rows = seqs * 2 * tok
    made = pl.pallas_call(
        functools.partial(tables, *dims),
        out_shape=(
            jax.ShapeDtypeStruct((4, rows, rows), jnp.bfloat16),
            jax.ShapeDtypeStruct((4, rows, 128), jnp.float32),
            jax.ShapeDtypeStruct((4, inner_rows, inner_rows), jnp.bfloat16),
            jax.ShapeDtypeStruct((4, inner_rows, 128), jnp.float32),
            jax.ShapeDtypeStruct((layers, 128, 512), jnp.bfloat16),
        ),
        in_specs=[smem],
        out_specs=(vmem,) * 5,
        compiler_params=pltpu.CompilerParams(vmem_limit_bytes=2**22),
        cost_estimate=pl.CostEstimate(flops=10**7, bytes_accessed=10**6, transcendentals=0),
        name="tables",
    )(place)
    weights = pltpu.VMEM((layers, 4, 1024, 128), jnp.bfloat16)
    result = pl.pallas_call(
        functools.partial(all_layers, dims),
        out_shape=jax.ShapeDtypeStruct((seqs * tok, width), jnp.bfloat16),
        in_specs=[smem] + [vmem] * 24,
        out_specs=vmem,
        scratch_shapes=[
            weights,
            weights,
            pltpu.VMEM((4, 512, 128), jnp.bfloat16),
            pltpu.VMEM((4, rows, width), jnp.bfloat16),
            pltpu.VMEM((4, layers, 128), jnp.float32),
        ],
        compiler_params=pltpu.CompilerParams(vmem_limit_bytes=18 * 2**20),
        cost_estimate=pl.CostEstimate(
            flops=2 * 10**9, bytes_accessed=18 * 10**6, transcendentals=1000
        ),
        name="all_layers",
    )(place, *p, *p_2, *q, *q_2, tokens, beside, gain, *made)
    return result.reshape(seqs, tok, width)


def solution(mesh):
    return jax.shard_map(
        body,
        mesh=mesh,
        in_specs=(
            P(None, "sp", "tp"),
            P(),
            P(None, "sp", "tp"),
            P(None, "tp", "sp"),
            P(None, "tp", "sp", None),
            P(None, "tp"),
        ),
        out_specs=P(None, "sp", "tp"),
        check_vma=False,
    )
```

```python
import functools

import jax
import jax.numpy as jnp
from jax import lax
from jax.experimental import pallas as pl
from jax.experimental.pallas import tpu as pltpu
from jax.sharding import PartitionSpec as P

NZ, NY, NC, NX = 4, 4, 2, 4
AXES = ("sp", "tp")


def flat(z, y, c, x):
    return (((z % NZ) * NY + y % NY) * NC + c) * NX + x % NX


def pairs(source_of):
    return [
        (flat(*source_of(z, y, c, x)), flat(z, y, c, x))
        for z in range(NZ)
        for y in range(NY)
        for c in range(NC)
        for x in range(NX)
    ]


FIRST = ("xzy", "zyx")
LAST = ("xyz", "yxz")


def along(order, step, k):
    def source(z, y, c, x):
        at = dict(z=z, y=y, x=x)
        at[order[c][step]] += k
        return at["z"], at["y"], c, at["x"]

    return pairs(source)


def gather(value, order, step):
    return [send(value, along(order, step, k)) for k in (1, 2, 3)]


def from_core():
    return pairs(lambda z, y, c, x: (z, y, 1 - c, x))


def across_chips():
    count = NZ * NY * NC
    swap = []
    for low in range(1, count - 1, 2):
        for x in range(NX):
            swap += [(low * NX + x, (low + 1) * NX + x), ((low + 1) * NX + x, low * NX + x)]
    return swap


def send(value, perm):
    return lax.ppermute(value, AXES, perm)


def copy_blocks(place, sources, order, copy):
    z, y, _, x = place
    for parts, core in sources:
        first = core == 0
        for k in range(4):
            for m in range(4):
                for j in range(4):
                    north, south = (dict(zip(axes, (j, m, k))) for axes in order)
                    y_at = lax.rem(y + jnp.where(first, north["y"], south["y"]), NY)
                    x_at = lax.rem(x + jnp.where(first, north["x"], south["x"]), NX)
                    z_at = lax.rem(z + jnp.where(first, north["z"], south["z"]), NZ)
                    copy(x_at, z_at * (NY * NC) + y_at * NC + core, parts[k].at[m, j])


def put_layers(layers, w_in, w_out, mix_raw=None):
    def copy(x_at, index, part):
        rows = pl.ds(pl.multiple_of(index * 32, 32), 32)
        for at, l in enumerate(layers):
            w_in[l, x_at, rows, :] = part[64 * at : 64 * at + 32, :]
            w_out[l, x_at, rows, :] = part[64 * at + 32 : 64 * at + 64, :]
        if mix_raw is not None:
            end = 64 * len(layers)
            mix_rows = pl.ds(pl.multiple_of(index * 16, 16), 16)
            mix_raw[x_at, mix_rows, :] = part[end : end + 16, :]

    return copy


def tables(layers, seqs, tok, halo, seq_len, place_ref, gain_ref, *refs):
    z, y, c = (place_ref[k] for k in range(3))
    first = ((z * NY + y) * NC + c) * tok
    for beside, bands, inverse in ((halo, *refs[0:2]), (halo // 2, *refs[2:4])):
        start = first - beside
        span = tok + 2 * beside
        rows = seqs * span
        r = lax.broadcasted_iota(jnp.int32, (rows, rows), 0)
        q = lax.broadcasted_iota(jnp.int32, (rows, rows), 1)
        same = (r >= span) == (q >= span)
        pos_r = start + jnp.where(r >= span, r - span, r)
        pos_q = start + jnp.where(q >= span, q - span, q)
        r1 = lax.broadcasted_iota(jnp.int32, (rows, 128), 0)
        pos_1 = start + jnp.where(r1 >= span, r1 - span, r1)
        for g in range(4):
            half = 2**g
            low = jnp.clip(pos_r - half, 0, seq_len)
            high = jnp.clip(pos_r + half, 0, seq_len)
            inside = same & (pos_q >= low) & (pos_q < high)
            bands[g] = jnp.where(inside, 1.0, 0.0).astype(jnp.bfloat16)
            count = jnp.clip(pos_1 + half, 0, seq_len) - jnp.clip(pos_1 - half, 0, seq_len)
            inverse[g] = 1.0 / jnp.maximum(count, 1).astype(jnp.float32)
    picks, gain = refs[4:6]
    gain[...] = gain_ref[...]
    pick_r = lax.broadcasted_iota(jnp.int32, (128, 512), 0)
    pick_q = lax.broadcasted_iota(jnp.int32, (128, 512), 1)
    base = ((pick_r >> 2) << 4) + (pick_r & 3)
    for l in range(layers):
        picks[l] = jnp.where(pick_q == base + 4 * l, 1.0, 0.0).astype(jnp.bfloat16)


def mix_layer(state, gain, w_in, scales, mixing, bands, inverse):
    mean = jnp.mean(state * state, axis=-1, keepdims=True)
    normed = (state * lax.rsqrt(mean + 1e-06) * gain).astype(jnp.bfloat16)
    weights = jnp.concatenate([w_in[g] for g in range(4)], axis=1)
    pooled = jnp.dot(normed, weights, preferred_element_type=jnp.float32).astype(jnp.bfloat16)
    mixed = []
    for g in range(4):
        part = pooled[:, 128 * g : 128 * (g + 1)]
        sums = jnp.dot(bands[g], part, preferred_element_type=jnp.float32)
        centred = (sums * inverse[g] - part.astype(jnp.float32)).astype(jnp.bfloat16)
        product = jnp.dot(
            centred, mixing[:, 128 * g : 128 * (g + 1)], preferred_element_type=jnp.float32
        )
        mixed.append((product * scales[g]).astype(jnp.bfloat16))
    return jnp.concatenate(mixed, axis=1)


def project_out(mixed, w_out):
    weights = jnp.concatenate([w_out(g) for g in range(4)], axis=1)
    out = lax.dot_general(
        mixed, weights, (((1,), (1,)), ((), ())), preferred_element_type=jnp.float32
    )
    return out.astype(jnp.bfloat16)


def inner(rows, seqs, cut):
    span = rows.shape[0] // seqs
    return jnp.concatenate([rows[s * span + cut : (s + 1) * span - cut] for s in range(seqs)])


def all_layers(dims, place_ref, *refs):
    layers, seqs, tok, halo, _ = dims
    tokens, beside = refs[16:18], refs[18]
    wide, narrow, picks, gain, out = refs[19:21], refs[21:23], refs[23], refs[24], refs[25]
    w_in, w_out, mix_raw, state_parts, scales = refs[26:]
    place = tuple(place_ref[k] for k in range(4))
    _, _, c, x = place
    span = tok + 2 * halo

    def place_tokens(acts):
        for k in range(4):
            x_at = lax.rem(x + k, NX)
            for h in range(2):
                lanes = slice(128 * h, 128 * (h + 1))
                for s in range(seqs):
                    for core in range(NC):
                        low = 80 + ((core * 2 + h) * seqs + s) * tok
                        at = pl.ds(pl.multiple_of(s * span + (1 + core - c) * tok, tok), tok)
                        state_parts[x_at, at, lanes] = acts[k, low : low + tok, :]
                    low = (h * seqs + s) * tok
                    at = pl.ds(pl.multiple_of(s * span + 2 * c * tok, tok), tok)
                    state_parts[x_at, at, lanes] = beside[k, low : low + tok, :]
            terms = acts[k, 64:80, :].astype(jnp.float32)
            scales[x_at] = (
                terms[0:layers] + terms[layers : 2 * layers] + terms[2 * layers : 3 * layers]
            )

    for core in range(NC):
        pl.when(c == core)(functools.partial(place_tokens, tokens[core]))
    put = put_layers(range(layers - 1), w_in, w_out, mix_raw)
    copy_blocks(place, ((refs[0:4], c), (refs[4:8], 1 - c)), FIRST, put)
    put = put_layers((layers - 1,), w_in, w_out)
    copy_blocks(place, ((refs[8:12], c), (refs[12:16], 1 - c)), LAST, put)

    raw = jnp.concatenate([mix_raw[g] for g in range(4)], axis=1)
    state = jnp.concatenate([state_parts[k] for k in range(4)], axis=1)
    for l in range(layers):
        mixing = jnp.dot(picks[l], raw, preferred_element_type=jnp.float32).astype(jnp.bfloat16)
        bands, inverse = wide if l < layers // 2 else narrow
        mixed = mix_layer(
            state.astype(jnp.float32),
            gain[l : l + 1, :],
            [w_in[l, g] for g in range(4)],
            [scales[g, l : l + 1, :] for g in range(4)],
            mixing,
            bands,
            inverse,
        )
        if l == layers // 2 - 1:
            mixed = inner(mixed, seqs, halo // 2)
        if l < layers - 1:
            state = project_out(mixed, lambda g: w_out[l, g])
        else:
            width = out.shape[-1]
            columns = pl.ds(pl.multiple_of(x * width, width), width)
            mixed = inner(mixed, seqs, halo // 2)
            out[...] = project_out(mixed, lambda g: w_out[l, g, columns, :])


def pack(
    layers, place_ref, in_ref, out_ref, mix_ref, scale_ref, act_ref, first, last
):
    for l in range(layers - 1):
        first[64 * l : 64 * l + 32, :] = in_ref[l]
        first[64 * l + 32 : 64 * l + 64, :] = out_ref[l]
    mix = jnp.concatenate([mix_ref[k].astype(jnp.float32) for k in range(layers)])
    first[64 * layers - 64 : 64 * layers - 48, :] = mix.astype(jnp.bfloat16)
    last[0:32, :] = in_ref[layers - 1]
    last[32:64, :] = out_ref[layers - 1]
    scale = scale_ref[...]
    high = scale.astype(jnp.bfloat16).astype(jnp.float32)
    middle = (scale - high).astype(jnp.bfloat16).astype(jnp.float32)
    terms = jnp.concatenate([high, middle, scale - high - middle, jnp.zeros_like(scale)])
    last[64:80, :] = terms.astype(jnp.bfloat16)
    seqs, tok, _ = act_ref.shape
    own = 80 + place_ref[2] * (seqs * tok * 2)
    for h in range(2):
        for s in range(seqs):
            at = pl.ds(pl.multiple_of(own + (h * seqs + s) * tok, 16), tok)
            last[at, :] = act_ref[s, :, 128 * h : 128 * (h + 1)]


def body(activations, norm_gain, in_weight, out_weight, mixing, pool_scale):
    layers = in_weight.shape[0]
    seqs, tok, width = activations.shape
    i, x = lax.axis_index("sp"), lax.axis_index("tp")
    z, y, c = i // (NY * NC), (i // NC) % NY, i % NC
    seq_len = tok * NZ * NY * NC
    chip_mate = send(activations, from_core())
    place = jnp.stack([z, y, c, x]).astype(jnp.int32)
    vmem = pl.BlockSpec(memory_space=pltpu.VMEM)
    smem = pl.BlockSpec(memory_space=pltpu.SMEM)
    first, last = pl.pallas_call(
        functools.partial(pack, layers),
        out_shape=(
            jax.ShapeDtypeStruct((64 * layers - 48, 128), jnp.bfloat16),
            jax.ShapeDtypeStruct((80 + 4 * seqs * tok, 128), jnp.bfloat16),
        ),
        in_specs=[smem] + [vmem] * 5,
        out_specs=(vmem, vmem),
        compiler_params=pltpu.CompilerParams(vmem_limit_bytes=2**21),
        cost_estimate=pl.CostEstimate(flops=10**6, bytes_accessed=3 * 10**5, transcendentals=0),
        name="pack",
    )(
        place,
        in_weight,
        jnp.swapaxes(out_weight, 1, 2),
        mixing.reshape(layers, 4, 128),
        pool_scale,
        activations,
    )
    mate_rows = jnp.concatenate(
        [chip_mate.reshape(seqs * tok, width)[:, 128 * h : 128 * (h + 1)] for h in range(2)]
    )
    count = 2 * seqs * tok
    last = lax.dynamic_update_slice(last, mate_rows, (80 + (1 - c) * count, 0))

    got = [first] + gather(first, FIRST, 0)
    got_last = [last] + gather(last, LAST, 0)
    p = jnp.stack(got)
    p = [p] + gather(p, FIRST, 1)
    q = jnp.stack([part[:64] for part in got_last])
    q = [q] + gather(q, LAST, 1)

    p = jnp.stack(p)
    p = [p] + gather(p, FIRST, 2)
    q = jnp.stack(q)
    q = [q] + gather(q, LAST, 2)
    tokens = jnp.stack(got_last)
    tokens_2 = send(tokens, from_core())
    mine = jnp.where(c == 0, tokens[:, 80 : 80 + count], tokens_2[:, 80 + count :])
    beside = send(mine, across_chips())
    p_2 = [send(p[0], from_core())]
    q_2 = [send(q[0], from_core())]
    p_2 += [send(part, from_core()) for part in p[1:]]
    q_2 += [send(part, from_core()) for part in q[1:]]

    rows = seqs * 3 * tok
    dims = (layers, seqs, tok, tok, seq_len)
    inner_rows = seqs * 2 * tok
    made = pl.pallas_call(
        functools.partial(tables, *dims),
        out_shape=(
            jax.ShapeDtypeStruct((4, rows, rows), jnp.bfloat16),
            jax.ShapeDtypeStruct((4, rows, 128), jnp.float32),
            jax.ShapeDtypeStruct((4, inner_rows, inner_rows), jnp.bfloat16),
            jax.ShapeDtypeStruct((4, inner_rows, 128), jnp.float32),
            jax.ShapeDtypeStruct((layers, 128, 512), jnp.bfloat16),
            jax.ShapeDtypeStruct(norm_gain.shape, jnp.float32),
        ),
        in_specs=[smem, vmem],
        out_specs=(vmem,) * 6,
        compiler_params=pltpu.CompilerParams(vmem_limit_bytes=2**22),
        cost_estimate=pl.CostEstimate(flops=10**7, bytes_accessed=10**6, transcendentals=0),
        name="tables",
    )(place, norm_gain)
    weights = pltpu.VMEM((layers, 4, 1024, 128), jnp.bfloat16)
    result = pl.pallas_call(
        functools.partial(all_layers, dims),
        out_shape=jax.ShapeDtypeStruct((seqs * tok, width), jnp.bfloat16),
        in_specs=[smem] + [vmem] * 25,
        out_specs=vmem,
        scratch_shapes=[
            weights,
            weights,
            pltpu.VMEM((4, 512, 128), jnp.bfloat16),
            pltpu.VMEM((4, rows, width), jnp.bfloat16),
            pltpu.VMEM((4, layers, 128), jnp.float32),
        ],
        compiler_params=pltpu.CompilerParams(vmem_limit_bytes=18 * 2**20),
        cost_estimate=pl.CostEstimate(
            flops=2 * 10**9, bytes_accessed=18 * 10**6, transcendentals=1000
        ),
        name="all_layers",
    )(place, *p, *p_2, *q, *q_2, tokens, tokens_2, beside, *made)
    return result.reshape(seqs, tok, width)


def solution(mesh):
    return jax.shard_map(
        body,
        mesh=mesh,
        in_specs=(
            P(None, "sp", "tp"),
            P(),
            P(None, "sp", "tp"),
            P(None, "tp", "sp"),
            P(None, "tp", "sp", None),
            P(None, "tp"),
        ),
        out_specs=P(None, "sp", "tp"),
        check_vma=False,
    )
```
